32 devices in a mesh: sp: 16 (over z, y, x), tp: 2 (over core).
Axes of the slice: x: 2, y: 2, z: 4, core: 2. Of those that a mesh axis runs over, the one named last changes fastest.
Arguments:
- tokens: bfloat16 [6144, 2048], P('sp', 'tp'), may hold values from -6 to 6
- input_gain: float32 [2048], replicated, may hold values from 0.1 to 1.9
- query_weight: bfloat16 [2048, 1024], P(None, 'tp'), may hold values from -0.5 to 0.5
- query_rot_weight: bfloat16 [2048, 512], P(None, 'tp'), may hold values from -0.125 to 0.125
- kv_down: bfloat16 [2048, 256], replicated, may hold values from -0.5 to 0.5
- rot_down: bfloat16 [2048, 32], replicated, may hold values from -0.125 to 0.125
- kv_gain: float32 [256], replicated, may hold values from 0.1 to 1.9
- key_up: bfloat16 [256, 1024], P(None, 'tp'), may hold values from -0.5 to 0.5
- value_up: bfloat16 [256, 1024], P(None, 'tp'), may hold values from -4 to 4
- conv_value_weight: bfloat16 [2048, 1024], P(None, 'tp'), may hold values from -0.125 to 0.125
- conv_gate_weight: bfloat16 [2048, 1024], P(None, 'tp'), may hold values from -0.125 to 0.125
- conv_taps: float32 [31, 1024], P(None, 'tp'), may hold values from -8 to 8
- conv_ln_gain: float32 [1024], P('tp'), may hold values from 0.1 to 1.9
- conv_ln_bias: float32 [1024], P('tp'), may hold values from -3 to 3
- att_out_gain: float32 [1024], P('tp'), may hold values from 0.1 to 1.9
- conv_out_gain: float32 [1024], P('tp'), may hold values from 0.1 to 1.9
- att_out_weight: bfloat16 [1024, 2048], P('tp'), may hold values from -0.125 to 0.125
- conv_out_weight: bfloat16 [1024, 2048], P('tp'), may hold values from -0.125 to 0.125
Outputs:
- mixed: bfloat16 [6144, 2048], P('sp', 'tp')
The draws below stay inside these ranges and needn't reach their ends.
All inputs are finite; a program needn't handle non-finite values.
Results may differ from the reference program's by a relative error of at most 0.017.
Values may be sent and summed in bfloat16 or wider, within the bound.
A program may use at most 128 MiB of HBM per device.

```python
import math
import jax
import jax.numpy as jnp
from jax import lax

D_MODEL = 2048
HEADS = 16
NOPE_DIM = 64
ROT_DIM = 32
VALUE_DIM = 64
KV_RANK = 256
CONV_CH = 1024
KERNEL = 31
TOKENS = 6144
ATT_WIDTH = 1024
N_TP = 2


def latent_weights(key):
    down_map = jax.random.normal(jax.random.fold_in(key, 101), (D_MODEL, KV_RANK), jnp.float32) / math.sqrt(D_MODEL)
    upward = jax.random.normal(jax.random.fold_in(key, 102), (KV_RANK, HEADS * NOPE_DIM), jnp.float32) / math.sqrt(KV_RANK)
    return (jnp.clip(down_map, -0.5, 0.5), jnp.clip(upward, -0.5, 0.5))


def rising_scales(key, entries):
    position = jnp.arange(entries, dtype=jnp.float32) / max(entries - 1, 1)
    jitter = jax.random.uniform(key, (entries,), jnp.float32)
    return 10.0 ** (0.5 * position + 0.5 * jitter - 0.5)


def draw_tokens(key, part):
    base_draw = jax.random.normal(jax.random.fold_in(key, 1), (TOKENS, D_MODEL), jnp.float32)
    return jnp.clip(base_draw, -6.0, 6.0).astype(jnp.bfloat16)


def draw_query_weight(key, part):
    base_draw = jax.random.normal(jax.random.fold_in(key, 104), (D_MODEL, HEADS * NOPE_DIM), jnp.float32) / math.sqrt(D_MODEL)
    return jnp.clip(base_draw, -0.5, 0.5).astype(jnp.bfloat16)


def draw_kv_down(key, part):
    return latent_weights(key)[0].astype(jnp.bfloat16)


def draw_key_up(key, part):
    return latent_weights(key)[1].astype(jnp.bfloat16)


def draw_value_up(key, part):
    base_draw = jax.random.normal(jax.random.fold_in(key, 201), (KV_RANK, HEADS * VALUE_DIM), jnp.float32) / math.sqrt(KV_RANK)
    scales = jnp.repeat(rising_scales(jax.random.fold_in(key, 202), HEADS), VALUE_DIM)
    return jnp.clip(base_draw * scales[None, :], -4.0, 4.0).astype(jnp.bfloat16)


def draw_conv_taps(key, part):
    base_draw = jax.random.normal(jax.random.fold_in(key, 301), (KERNEL, CONV_CH), jnp.float32) / math.sqrt(KERNEL)
    scales = rising_scales(jax.random.fold_in(key, 302), CONV_CH)
    return jnp.clip(base_draw * scales[None, :], -8.0, 8.0).astype(jnp.float32)


def steps_of(stream_key, dims, shards, least, largest):
    def one(dim, parts):
        heights = jax.random.uniform(jax.random.fold_in(jax.random.fold_in(stream_key, 6), dim), (parts,), jnp.float32, least / len(shards), largest / len(shards))
        return jnp.repeat(jnp.exp(heights), dims[dim] // parts).reshape((-1,) + (1,) * (len(dims) - dim - 1))

    level = one(*shards[0])
    for cut in shards[1:]:
        level = level * one(*cut)
    return level


def centred(own_key, dims, width, limit, split=(), held_as=jnp.bfloat16):
    values = width * jax.random.normal(own_key, dims, jnp.float32)
    if split:
        values = values * steps_of(own_key, dims, split, -0.22, 0.18)
    return jnp.clip(values, -limit, limit).astype(held_as)


def setup_inputs(seed: int = 0) -> dict:
    key_of = jax.random.split(jax.random.key(seed), 19)
    tokens = draw_tokens(jax.random.fold_in(key_of[18], 71), 0)
    input_gain = jnp.clip(1.0 + 0.18 * jax.random.normal(key_of[1], (D_MODEL,), jnp.float32), 0.1, 1.9)
    query_weight = draw_query_weight(jax.random.fold_in(key_of[18], 71), 0)
    query_rot_weight = centred(key_of[3], (D_MODEL, HEADS * ROT_DIM), D_MODEL ** -0.5, 0.125, ((1, 2),))
    kv_down = draw_kv_down(jax.random.fold_in(key_of[18], 71), 0)
    rot_down = centred(key_of[5], (D_MODEL, ROT_DIM), D_MODEL ** -0.5, 0.125)
    kv_gain = jnp.clip(1.0 + 0.18 * jax.random.normal(key_of[6], (KV_RANK,), jnp.float32), 0.1, 1.9)
    key_up = draw_key_up(jax.random.fold_in(key_of[18], 71), 0)
    value_up = draw_value_up(jax.random.fold_in(key_of[18], 71), 0)
    conv_value_weight = centred(key_of[9], (D_MODEL, CONV_CH), D_MODEL ** -0.5, 0.125, ((1, 2),))
    conv_gate_weight = centred(key_of[10], (D_MODEL, CONV_CH), D_MODEL ** -0.5, 0.125, ((1, 2),))
    conv_taps = draw_conv_taps(jax.random.fold_in(key_of[18], 71), 0)
    conv_ln_gain = jnp.clip(1.0 + 0.18 * jax.random.normal(key_of[12], (CONV_CH,), jnp.float32), 0.1, 1.9)
    conv_ln_bias = centred(key_of[13], (CONV_CH,), 0.5, 3.0, ((0, 2),), jnp.float32)
    att_out_gain = jnp.clip(1.0 + 0.18 * jax.random.normal(key_of[14], (ATT_WIDTH,), jnp.float32), 0.1, 1.9)
    conv_out_gain = jnp.clip(1.0 + 0.18 * jax.random.normal(key_of[15], (CONV_CH,), jnp.float32), 0.1, 1.9)
    att_out_weight = centred(key_of[16], (ATT_WIDTH, D_MODEL), (ATT_WIDTH + CONV_CH) ** -0.5, 0.125, ((0, 2),))
    conv_out_weight = centred(key_of[17], (CONV_CH, D_MODEL), (ATT_WIDTH + CONV_CH) ** -0.5, 0.125, ((0, 2),))
    return {"tokens": tokens, "input_gain": input_gain, "query_weight": query_weight, "query_rot_weight": query_rot_weight, "kv_down": kv_down, "rot_down": rot_down, "kv_gain": kv_gain, "key_up": key_up, "value_up": value_up, "conv_value_weight": conv_value_weight, "conv_gate_weight": conv_gate_weight, "conv_taps": conv_taps, "conv_ln_gain": conv_ln_gain, "conv_ln_bias": conv_ln_bias, "att_out_gain": att_out_gain, "conv_out_gain": conv_out_gain, "att_out_weight": att_out_weight, "conv_out_weight": conv_out_weight}


norm_eps = 1e-06
rope_base = 10000.0

def lifted(array):
    return lax.optimization_barrier(array).astype(jnp.float32)

def rotary_tables(positions, half_dim):
    frequency = rope_base ** (-jnp.arange(half_dim, dtype=jnp.float32) / half_dim)
    angles = positions.astype(jnp.float32)[:, None] * frequency[None, :]
    return (jnp.cos(angles), jnp.sin(angles))

def rotate_half(values, cos_table, sine_table):
    half_dim = cos_table.shape[-1]
    front_half = values[..., :half_dim]
    back_half = values[..., half_dim:]
    return jnp.concatenate([front_half * cos_table - back_half * sine_table, back_half * cos_table + front_half * sine_table], axis=-1)

def reference(tokens, input_gain, query_weight, query_rot_weight, kv_down, rot_down, kv_gain, key_up, value_up, conv_value_weight, conv_gate_weight, conv_taps, conv_ln_gain, conv_ln_bias, att_out_gain, conv_out_gain, att_out_weight, conv_out_weight):
    tokens_wide = tokens.astype(jnp.float32)
    row_scale = lax.rsqrt(lax.optimization_barrier(jnp.mean(tokens_wide * tokens_wide, axis=1, keepdims=True)) + norm_eps)
    scaled = (tokens_wide * input_gain[None, :]).astype(jnp.bfloat16)

    def project(weight):
        return jnp.dot(scaled.astype(jnp.float32), weight.astype(jnp.float32), preferred_element_type=jnp.float32)
    positions = jnp.arange(TOKENS, dtype=jnp.int32)
    cos_table, sine_table = rotary_tables(positions, ROT_DIM // 2)
    queries = (project(query_weight) * row_scale).astype(jnp.bfloat16).reshape(TOKENS, HEADS, NOPE_DIM)
    query_rot = rotate_half((project(query_rot_weight) * row_scale).reshape(TOKENS, HEADS, ROT_DIM), cos_table[:, None, :], sine_table[:, None, :]).astype(jnp.bfloat16)
    latent_raw = project(kv_down)
    latent = (latent_raw * lax.rsqrt(lax.optimization_barrier(jnp.mean(latent_raw * latent_raw, axis=1, keepdims=True)) + norm_eps) * kv_gain[None, :]).astype(jnp.bfloat16)
    key_rot = rotate_half(project(rot_down) * row_scale, cos_table, sine_table).astype(jnp.bfloat16)
    keys = jnp.dot(latent.astype(jnp.float32), key_up.astype(jnp.float32), preferred_element_type=jnp.float32).astype(jnp.bfloat16).reshape(TOKENS, HEADS, NOPE_DIM)
    values = jnp.dot(latent.astype(jnp.float32), value_up.astype(jnp.float32), preferred_element_type=jnp.float32).astype(jnp.bfloat16).reshape(TOKENS, HEADS, VALUE_DIM)
    queries_heads = jnp.transpose(lifted(queries), (1, 0, 2))
    qrot_heads = jnp.transpose(lifted(query_rot), (1, 0, 2))
    keys_heads = jnp.transpose(lifted(keys), (1, 0, 2))
    values_heads = jnp.transpose(lifted(values), (1, 0, 2))
    krot_wide = lifted(key_rot)
    inv_scale = 1.0 / math.sqrt(NOPE_DIM + ROT_DIM)
    block_len = min(512, TOKENS)
    pieces = []
    for block_idx in range(TOKENS // block_len):
        row_low = block_idx * block_len
        row_high = row_low + block_len
        key_pos = jnp.arange(row_high, dtype=jnp.int32)
        query_pos = jnp.arange(row_low, row_high, dtype=jnp.int32)
        visible = key_pos[None, :] <= query_pos[:, None]
        krot_part = krot_wide[:row_high]

        def one_head(members):
            query_head, qrot_head, key_head, value_head = members
            scores = (jnp.dot(query_head, key_head.T) + jnp.dot(qrot_head, krot_part.T)) * inv_scale
            row_max = lax.optimization_barrier(jnp.max(jnp.where(visible, scores, -jnp.inf), axis=1, keepdims=True))
            exp_scores = jnp.where(visible, jnp.exp(scores - row_max), 0.0)
            denominator = lax.optimization_barrier(jnp.sum(exp_scores, axis=1, keepdims=True))
            weighted = jnp.dot(lifted(exp_scores.astype(jnp.bfloat16)), value_head)
            return weighted / denominator
        head_out = lax.map(one_head, (queries_heads[:, row_low:row_high], qrot_heads[:, row_low:row_high], keys_heads[:, :row_high], values_heads[:, :row_high]))
        pieces.append(jnp.transpose(head_out, (1, 0, 2)).astype(jnp.bfloat16))
    attended = jnp.concatenate(pieces, axis=0).reshape(TOKENS, ATT_WIDTH)
    gated_input = (project(conv_value_weight) * row_scale * jax.nn.sigmoid(project(conv_gate_weight) * row_scale)).astype(jnp.bfloat16)
    padded = jnp.pad(lifted(gated_input), ((KERNEL - 1, 0), (0, 0)))
    conv_out = jnp.zeros((TOKENS, CONV_CH), jnp.float32)
    for tap_idx in range(KERNEL):
        conv_out = conv_out + conv_taps[tap_idx][None, :] * padded[tap_idx:tap_idx + TOKENS]
    mean_val = lax.optimization_barrier(jnp.mean(conv_out, axis=1, keepdims=True))
    spread = lax.optimization_barrier(jnp.mean(conv_out * conv_out, axis=1, keepdims=True)) - mean_val * mean_val
    swished = jax.nn.silu((conv_out - mean_val) * lax.rsqrt(spread + norm_eps) * conv_ln_gain[None, :] + conv_ln_bias[None, :])
    conv_mixed = (swished * lax.rsqrt(lax.optimization_barrier(jnp.mean(swished * swished, axis=1, keepdims=True)) + norm_eps) * conv_out_gain[None, :]).astype(jnp.bfloat16)
    att_wide = lifted(attended)
    att_mixed = (att_wide * lax.rsqrt(lax.optimization_barrier(jnp.mean(att_wide * att_wide, axis=1, keepdims=True)) + norm_eps) * att_out_gain[None, :]).astype(jnp.bfloat16)
    att_share = ATT_WIDTH // N_TP
    conv_share = CONV_CH // N_TP
    result = jnp.zeros((TOKENS, D_MODEL), jnp.float32)
    for group_idx in range(N_TP):
        att_low = group_idx * att_share
        conv_low = group_idx * conv_share
        partial_value = jnp.dot(att_mixed[:, att_low:att_low + att_share].astype(jnp.float32), att_out_weight[att_low:att_low + att_share].astype(jnp.float32), preferred_element_type=jnp.float32) + jnp.dot(conv_mixed[:, conv_low:conv_low + conv_share].astype(jnp.float32), conv_out_weight[conv_low:conv_low + conv_share].astype(jnp.float32), preferred_element_type=jnp.float32)
        result = result + lifted(partial_value.astype(jnp.bfloat16))
    return result.astype(jnp.bfloat16)
```

```python
import math

import jax
import jax.numpy as jnp
from jax import lax
from jax.experimental import pallas as pl
from jax.experimental.pallas import tpu as pltpu
from jax.sharding import PartitionSpec as P

D_MODEL = 2048
NOPE_DIM = 64
ROT_DIM = 32
VALUE_DIM = 64
CONV_CH = 1024
KERNEL = 31
ATT_WIDTH = 1024


norm_eps = 1e-06
far_below = -1e30
rope_base = 10000.0


def shifted(block, axis, distance):
    devices = range(lax.axis_size(axis))
    route = [(i - distance, i) for i in devices if i - distance in devices]
    return lax.ppermute(block, axis, route)


def rotary_tables(positions, half_dim):
    frequency = rope_base ** (-jnp.arange(half_dim, dtype=jnp.float32) / half_dim)
    angles = positions.astype(jnp.float32)[:, None] * frequency[None, :]
    return (jnp.cos(angles), jnp.sin(angles))


def rotate_half(values, cos_table, sine_table):
    half_dim = cos_table.shape[-1]
    front_half = values[..., :half_dim]
    back_half = values[..., half_dim:]
    return jnp.concatenate(
        [
            front_half * cos_table - back_half * sine_table,
            back_half * cos_table + front_half * sine_table,
        ],
        axis=-1,
    )


def attention_kernel(q_ref, lat_ref, kup_ref, vup_ref, o_ref, kt, vt, run_max, acc):
    heads, rows, lanes = q_ref.shape
    blocks = lat_ref.shape[0]
    rank = kup_ref.shape[1]
    nope = kup_ref.shape[0] // heads
    vdim = vup_ref.shape[0] // heads
    rot = lat_ref.shape[1] - rank
    wide = kt.shape[2]
    group = wide // rows
    me = lax.axis_index("sp")
    last = me // group
    kt[:, nope + rot :, :] = jnp.zeros((heads, lanes - nope - rot, wide), jnp.bfloat16)
    vt[:, vdim:, :] = jnp.ones((heads, lanes - vdim, wide), jnp.bfloat16)

    def expand(block):
        for part in range(group):
            src = jnp.minimum(block * group + part, blocks - 1)
            lat = lat_ref[src, :rank, :]
            turned = lat_ref[src, rank:, :]
            cols = slice(part * rows, (part + 1) * rows)
            keys = jnp.dot(kup_ref[...], lat, preferred_element_type=jnp.float32)
            values = jnp.dot(vup_ref[...], lat, preferred_element_type=jnp.float32)
            for head in range(heads):
                kt[head, :nope, cols] = keys[head * nope : (head + 1) * nope].astype(jnp.bfloat16)
                kt[head, nope : nope + rot, cols] = turned
                vt[head, :vdim, cols] = values[head * vdim : (head + 1) * vdim].astype(
                    jnp.bfloat16
                )

    def weigh(head, scores, top):
        weights = jnp.exp2(scores - top).astype(jnp.bfloat16)
        return lax.dot_general(
            weights, vt[head], (((1,), (1,)), ((), ())), preferred_element_type=jnp.float32
        )

    expand(last)
    key_pos = last * wide + lax.broadcasted_iota(jnp.int32, (rows, wide), 1)
    query_pos = me * rows + lax.broadcasted_iota(jnp.int32, (rows, wide), 0)
    hidden = key_pos > query_pos
    for head in range(heads):
        scores = jnp.dot(q_ref[head], kt[head], preferred_element_type=jnp.float32)
        scores = jnp.where(hidden, far_below, scores)
        top = jnp.max(scores, axis=1, keepdims=True)
        run_max[head] = jnp.broadcast_to(top, (rows, lanes))
        acc[head] = weigh(head, scores, top)

    def visit(step, carry):
        expand(step)
        for head in range(heads):
            scores = jnp.dot(q_ref[head], kt[head], preferred_element_type=jnp.float32)
            old = run_max[head]
            top = jnp.maximum(old[:, :1], jnp.max(scores, axis=1, keepdims=True))
            wide_top = jnp.broadcast_to(top, (rows, lanes))
            run_max[head] = wide_top
            acc[head] = acc[head] * jnp.exp2(old - wide_top) + weigh(head, scores, top)
        return carry

    lax.fori_loop(0, last, visit, 0)
    lane = lax.broadcasted_iota(jnp.int32, (rows, lanes), 1)
    for pair in range(heads // 2):
        halves = []
        for head in (2 * pair, 2 * pair + 1):
            total = acc[head]
            halves.append(total / pltpu.roll(total, vdim, axis=1))
        both = jnp.where(lane < vdim, halves[0], pltpu.roll(halves[1], vdim, axis=1))
        o_ref[:, pair * lanes : (pair + 1) * lanes] = both.astype(jnp.bfloat16)


def attention(q_heads, lat_all, key_up_t, value_up_t):
    heads, rows, lanes = q_heads.shape
    blocks = lat_all.shape[0]
    wide = 2 * rows if blocks % 2 == 0 else rows
    vmem = pl.BlockSpec(memory_space=pltpu.VMEM)
    return pl.pallas_call(
        attention_kernel,
        out_shape=jax.ShapeDtypeStruct((rows, value_up_t.shape[0]), jnp.bfloat16),
        in_specs=[vmem] * 4,
        out_specs=vmem,
        scratch_shapes=[
            pltpu.VMEM((heads, lanes, wide), jnp.bfloat16),
            pltpu.VMEM((heads, lanes, wide), jnp.bfloat16),
            pltpu.VMEM((heads, rows, lanes), jnp.float32),
            pltpu.VMEM((heads, rows, lanes), jnp.float32),
        ],
        compiler_params=pltpu.CompilerParams(vmem_limit_bytes=48 << 20),
        cost_estimate=pl.CostEstimate(
            flops=20_000_000_000, bytes_accessed=8 << 20, transcendentals=20_000_000
        ),
        name="attention",
    )(q_heads, lat_all, key_up_t, value_up_t)


def conv_kernel(gated_ref, rim_ref, taps_ref, out_ref, wide):
    rows, chans = gated_ref.shape
    rim = rim_ref.shape[0]
    taps = taps_ref.shape[0]
    chunk = 64
    for part in range(chans // 128):
        cols = slice(part * 128, (part + 1) * 128)
        wide[part, :rim, :] = rim_ref[:, cols].astype(jnp.float32)
        wide[part, rim:, :] = gated_ref[:, cols].astype(jnp.float32)
        coeff = taps_ref[:, cols]

        def band(step, carry):
            base = step * chunk
            total = jnp.zeros((chunk, 128), jnp.float32)
            for tap in range(taps):
                total = total + coeff[tap : tap + 1, :] * wide[
                    part, pl.ds(base + (rim - taps + 1 + tap), chunk), :
                ]
            out_ref[pl.ds(pl.multiple_of(base, chunk), chunk), cols] = total
            return carry

        lax.fori_loop(0, rows // chunk, band, 0)


def convolve(gated, rim, taps):
    rows, chans = gated.shape
    vmem = pl.BlockSpec(memory_space=pltpu.VMEM)
    return pl.pallas_call(
        conv_kernel,
        out_shape=jax.ShapeDtypeStruct((rows, chans), jnp.float32),
        in_specs=[vmem] * 3,
        out_specs=vmem,
        scratch_shapes=[pltpu.VMEM((chans // 128, rows + rim.shape[0], 128), jnp.float32)],
        cost_estimate=pl.CostEstimate(
            flops=2 * rows * chans * 31, bytes_accessed=2 << 20, transcendentals=0
        ),
        name="depthwise",
    )(gated, rim, taps)


def shards(
    tokens,
    input_gain,
    query_weight,
    query_rot_weight,
    kv_down,
    rot_down,
    kv_gain,
    key_up,
    value_up,
    conv_value_weight,
    conv_gate_weight,
    conv_taps,
    conv_ln_gain,
    conv_ln_bias,
    att_out_gain,
    conv_out_gain,
    att_out_weight,
    conv_out_weight,
):
    tok_rows = tokens.shape[0]
    heads_here = key_up.shape[1] // NOPE_DIM
    chan_here = conv_taps.shape[1]
    weight_list = (
        query_weight,
        query_rot_weight,
        kv_down,
        rot_down,
        conv_value_weight,
        conv_gate_weight,
    )
    wide_part = lax.all_gather(tokens, "tp", axis=1, tiled=True).astype(jnp.float32)
    scaled = (wide_part * input_gain[None, :]).astype(jnp.bfloat16)

    def add_product(weight):
        return jnp.dot(scaled, weight, preferred_element_type=jnp.float32)

    summed = tuple((add_product(weight) for weight in weight_list))
    q_acc, qrot_acc, latent_raw, rot_acc, value_acc, gate_acc, square_sum = summed + (
        jnp.sum(wide_part * wide_part, axis=1),
    )
    row_scale = lax.rsqrt(square_sum / D_MODEL + norm_eps)[:, None]
    positions = lax.axis_index("sp") * tok_rows + jnp.arange(tok_rows, dtype=jnp.int32)
    cos_table, sine_table = rotary_tables(positions, ROT_DIM // 2)
    fold = math.log2(math.e) / math.sqrt(NOPE_DIM + ROT_DIM)
    query_scale = row_scale * fold
    plain_q = (q_acc * query_scale).reshape(tok_rows, heads_here, NOPE_DIM)
    turned_q = rotate_half(
        (qrot_acc * query_scale).reshape(tok_rows, heads_here, ROT_DIM),
        cos_table[:, None, :],
        sine_table[:, None, :],
    )
    blank = jnp.zeros((tok_rows, heads_here, 128 - NOPE_DIM - ROT_DIM), jnp.float32)
    q_heads = jnp.transpose(
        jnp.concatenate([plain_q, turned_q, blank], axis=2).astype(jnp.bfloat16), (1, 0, 2)
    )
    latent = (
        latent_raw
        * lax.rsqrt(jnp.mean(latent_raw * latent_raw, axis=1, keepdims=True) + norm_eps)
        * kv_gain[None, :]
    ).astype(jnp.bfloat16)
    key_rot = rotate_half(rot_acc * row_scale, cos_table, sine_table).astype(jnp.bfloat16)
    gated_input = (value_acc * row_scale * jax.nn.sigmoid(gate_acc * row_scale)).astype(
        jnp.bfloat16
    )
    def square_rows(matrix):
        wide_rows = matrix.astype(jnp.float32)
        return jnp.sum(wide_rows * wide_rows, axis=1)

    packed = jnp.concatenate([latent.T, key_rot.T], axis=0)
    lat_all = lax.all_gather(packed, "sp", axis=0)
    rim_rows = shifted(gated_input[tok_rows - (KERNEL + 1) :], "sp", 1)
    conv_out = convolve(gated_input, rim_rows, conv_taps)
    attended = attention(q_heads, lat_all, key_up.T, value_up.T)
    att_sq = lax.psum(square_rows(attended), "tp")
    moment_one, moment_two = lax.psum(
        (jnp.sum(conv_out, axis=1), jnp.sum(conv_out * conv_out, axis=1)), "tp"
    )
    mean_val = moment_one / CONV_CH
    spread = moment_two / CONV_CH - mean_val * mean_val
    normed = (conv_out - mean_val[:, None]) * lax.rsqrt(spread + norm_eps)[:, None]
    swished = jax.nn.silu(normed * conv_ln_gain[None, :] + conv_ln_bias[None, :])
    conv_sq = lax.psum(square_rows(swished), "tp")
    att_mixed = (
        attended.astype(jnp.float32)
        * lax.rsqrt(att_sq / ATT_WIDTH + norm_eps)[:, None]
        * att_out_gain[None, :]
    ).astype(jnp.bfloat16)
    conv_mixed = (
        swished * lax.rsqrt(conv_sq / CONV_CH + norm_eps)[:, None] * conv_out_gain[None, :]
    ).astype(jnp.bfloat16)
    contract = (((0,), (1,)), ((), ()))
    feature_rows = lax.psum_scatter(
        (
            lax.dot_general(att_out_weight, att_mixed, contract, preferred_element_type=jnp.float32)
            + lax.dot_general(
                conv_out_weight, conv_mixed, contract, preferred_element_type=jnp.float32
            )
        ).astype(jnp.bfloat16),
        "tp",
        scatter_dimension=0,
        tiled=True,
    ).astype(jnp.float32)
    return feature_rows.T.astype(jnp.bfloat16)


def solution(mesh):
    return jax.shard_map(
        shards,
        mesh=mesh,
        in_specs=(
            P("sp", "tp"),
            P(),
            P(None, "tp"),
            P(None, "tp"),
            P(),
            P(),
            P(),
            P(None, "tp"),
            P(None, "tp"),
            P(None, "tp"),
            P(None, "tp"),
            P(None, "tp"),
            P("tp"),
            P("tp"),
            P("tp"),
            P("tp"),
            P("tp", None),
            P("tp", None),
        ),
        out_specs=P("sp", "tp"),
        check_vma=False,
    )
```

```python
import math

import jax
import jax.numpy as jnp
from jax import lax
from jax.experimental import pallas as pl
from jax.experimental.pallas import tpu as pltpu
from jax.sharding import PartitionSpec as P

D_MODEL = 2048
NOPE_DIM = 64
ROT_DIM = 32
VALUE_DIM = 64
CONV_CH = 1024
KERNEL = 31
ATT_WIDTH = 1024


norm_eps = 1e-06
far_below = -1e30
rope_base = 10000.0


def shifted(block, axis, distance):
    devices = range(lax.axis_size(axis))
    route = [(i - distance, i) for i in devices if i - distance in devices]
    return lax.ppermute(block, axis, route)


def rotary_tables(positions, half_dim):
    frequency = rope_base ** (-jnp.arange(half_dim, dtype=jnp.float32) / half_dim)
    angles = positions.astype(jnp.float32)[:, None] * frequency[None, :]
    return (jnp.cos(angles), jnp.sin(angles))


def rotate_half(values, cos_table, sine_table):
    half_dim = cos_table.shape[-1]
    front_half = values[..., :half_dim]
    back_half = values[..., half_dim:]
    return jnp.concatenate(
        [
            front_half * cos_table - back_half * sine_table,
            back_half * cos_table + front_half * sine_table,
        ],
        axis=-1,
    )


MESH = pl.DeviceIdType.MESH


def push(src, dst, send, recv, target):
    return pltpu.make_async_remote_copy(
        src_ref=src,
        dst_ref=dst,
        send_sem=send,
        recv_sem=recv,
        device_id=target,
        device_id_type=MESH,
    )


def greet(targets):
    barrier = pltpu.get_barrier_semaphore()
    for target in targets:
        pl.semaphore_signal(barrier, inc=1, device_id=target, device_id_type=MESH)
    pl.semaphore_wait(barrier, len(targets))


def other_core():
    return {"sp": lax.axis_index("sp"), "tp": 1 - lax.axis_index("tp")}


def tokens_kernel(tok_ref, gain_ref, scaled_ref, scale_ref, landed, send, recv):
    mine = lax.axis_index("tp")
    width = tok_ref.shape[1]
    greet([other_core()])
    copy = push(tok_ref, landed, send, recv, other_core())
    copy.start()

    def place(block, index):
        cols = pl.ds(pl.multiple_of(index * width, 128), width)
        wide = block[...].astype(jnp.float32)
        scaled_ref[:, cols] = (wide * gain_ref[:, cols]).astype(jnp.bfloat16)
        return jnp.sum(wide * wide, axis=1, keepdims=True)

    squares = place(tok_ref, mine)
    copy.wait()
    squares = squares + place(landed, 1 - mine)
    scale_ref[...] = lax.rsqrt(squares / (2 * width) + norm_eps)


def exchange_tokens(tokens, gain):
    rows, width = tokens.shape
    vmem = pl.BlockSpec(memory_space=pltpu.VMEM)
    return pl.pallas_call(
        tokens_kernel,
        out_shape=(
            jax.ShapeDtypeStruct((rows, 2 * width), jnp.bfloat16),
            jax.ShapeDtypeStruct((rows, 1), jnp.float32),
        ),
        in_specs=[vmem] * 2,
        out_specs=(vmem, vmem),
        scratch_shapes=[
            pltpu.VMEM((rows, width), jnp.bfloat16),
            pltpu.SemaphoreType.DMA,
            pltpu.SemaphoreType.DMA,
        ],
        compiler_params=pltpu.CompilerParams(collective_id=0, has_side_effects=True),
        name="token_exchange",
    )(tokens, gain)


def output_kernel(
    att_ref, swish_ref, att_gain, conv_gain, att_w, conv_w, out_ref,
    sq_mine, sq_other, part, landed, sq_send, sq_recv, send, recv,
):
    mine = lax.axis_index("tp")
    rows, width = out_ref.shape
    lanes = sq_mine.shape[1] // 2
    attended = att_ref[...].astype(jnp.float32)
    swished = swish_ref[...]
    for slot, value in enumerate((attended, swished)):
        total = jnp.sum(value * value, axis=1, keepdims=True)
        sq_mine[:, slot * lanes : (slot + 1) * lanes] = jnp.broadcast_to(total, (rows, lanes))
    greet([other_core()])
    sums = push(sq_mine, sq_other, sq_send, sq_recv, other_core())
    sums.start()
    sums.wait()
    sq = sq_mine[...] + sq_other[...]
    att_scale = lax.rsqrt(sq[:, :1] / ATT_WIDTH + norm_eps)
    conv_scale = lax.rsqrt(sq[:, lanes : lanes + 1] / CONV_CH + norm_eps)
    att_mixed = (attended * att_scale * att_gain[...]).astype(jnp.bfloat16)
    conv_mixed = (swished * conv_scale * conv_gain[...]).astype(jnp.bfloat16)
    piece = part.shape[2]
    pieces = part.shape[0]

    def product(owner, index):
        cols = pl.ds(pl.multiple_of(owner * width + index * piece, 128), piece)
        return (
            jnp.dot(att_mixed, att_w[:, cols], preferred_element_type=jnp.float32)
            + jnp.dot(conv_mixed, conv_w[:, cols], preferred_element_type=jnp.float32)
        ).astype(jnp.bfloat16)

    copies = []
    for index in range(pieces):
        part[index] = product(1 - mine, index)
        copy = push(
            part.at[index], landed.at[index], send.at[index], recv.at[index], other_core()
        )
        copy.start()
        copies.append(copy)
    for index in range(pieces):
        own = product(mine, index).astype(jnp.float32)
        copies[index].wait()
        out_ref[:, index * piece : (index + 1) * piece] = (
            own + landed[index].astype(jnp.float32)
        ).astype(jnp.bfloat16)


def merge(attended, swished, att_gain, conv_gain, att_w, conv_w):
    rows = attended.shape[0]
    width = att_w.shape[1] // 2
    pieces = 4
    vmem = pl.BlockSpec(memory_space=pltpu.VMEM)
    return pl.pallas_call(
        output_kernel,
        out_shape=jax.ShapeDtypeStruct((rows, width), jnp.bfloat16),
        in_specs=[vmem] * 6,
        out_specs=vmem,
        scratch_shapes=[
            pltpu.VMEM((rows, 256), jnp.float32),
            pltpu.VMEM((rows, 256), jnp.float32),
            pltpu.VMEM((pieces, rows, width // pieces), jnp.bfloat16),
            pltpu.VMEM((pieces, rows, width // pieces), jnp.bfloat16),
            pltpu.SemaphoreType.DMA,
            pltpu.SemaphoreType.DMA,
            pltpu.SemaphoreType.DMA((pieces,)),
            pltpu.SemaphoreType.DMA((pieces,)),
        ],
        compiler_params=pltpu.CompilerParams(collective_id=1, has_side_effects=True),
        name="output_merge",
    )(attended, swished, att_gain, conv_gain, att_w, conv_w)


PLANE = 4


def attention_kernel(
    q_ref, own_ref, kup_ref, vup_ref, o_ref, kt, vt, run_max, acc, lat_ref,
    col_send, plane_send, core_send, link_recv, core_recv,
):
    heads, rows, lanes = q_ref.shape
    blocks = lat_ref.shape[0]
    rank = kup_ref.shape[1]
    nope = kup_ref.shape[0] // heads
    vdim = vup_ref.shape[0] // heads
    rot = lat_ref.shape[1] - rank
    wide = kt.shape[2]
    pairing = wide // rows
    me = lax.axis_index("sp")
    core = lax.axis_index("tp")
    layers = blocks // PLANE
    layer = me // PLANE
    spot = me % PLANE
    last = me // pairing
    height = lat_ref.shape[1] // 2
    half = pl.ds(pl.multiple_of(core * height, 16), height)

    def spot_at(distance):
        return (spot + distance) % PLANE

    def at(layer_id, spot_id):
        return {"sp": layer_id * PLANE + spot_id, "tp": core}

    greet(
        [at((layer + d) % layers, spot) for d in range(1, layers)]
        + [at(layer, spot_at(d)) for d in range(1, PLANE)]
        + [other_core()]
    )

    def column_copy(distance):
        return push(
            own_ref.at[half],
            lat_ref.at[me, half],
            col_send.at[distance - 1],
            link_recv.at[me],
            at(jnp.minimum(layer + distance, layers - 1), spot),
        )

    def plane_copy(source, block, distance):
        return push(
            source,
            lat_ref.at[block, half],
            plane_send.at[block // PLANE, distance - 1],
            link_recv.at[block],
            at(layer, spot_at(distance)),
        )

    def core_copy(block):
        spread = lat_ref.at[block, half]
        return push(spread, spread, core_send.at[block], core_recv.at[block], other_core())

    for d in range(1, PLANE):
        plane_copy(own_ref.at[half], me, d).start()
    for d in range(1, layers):

        @pl.when(layer + d < layers)
        def _(d=d):
            column_copy(d).start()

    lat_ref[me] = own_ref[...]

    def relay(step):
        @pl.when(step <= layer)
        def _():
            block = (layer - step) * PLANE + spot
            landed(block)
            for d in range(1, PLANE):
                plane_copy(lat_ref.at[block, half], block, d).start()
            core_copy(block).start()

    def hand_over(step):
        @pl.when(step <= layer)
        def _():
            for d in range(1, PLANE):
                block = (layer - step) * PLANE + spot_at(d)
                landed(block)
                core_copy(block).start()

    def landed(block):
        spread = lat_ref.at[block, half]
        push(spread, spread, core_send.at[block], link_recv.at[block], other_core()).wait_recv()

    def gathered(step):
        for d in range(1, PLANE):
            core_copy((layer - step) * PLANE + spot_at(d)).wait_recv()

    def expand(pair):
        for part in range(pairing):
            src = pair * pairing + part
            lat = lat_ref[src, :rank, :]
            turned = lat_ref[src, rank:, :]
            cols = slice(part * rows, (part + 1) * rows)
            keys = jnp.dot(kup_ref[...], lat, preferred_element_type=jnp.float32)
            values = jnp.dot(vup_ref[...], lat, preferred_element_type=jnp.float32)
            for head in range(heads):
                kt[head, :nope, cols] = keys[head * nope : (head + 1) * nope].astype(jnp.bfloat16)
                kt[head, nope : nope + rot, cols] = turned
                vt[head, :vdim, cols] = values[head * vdim : (head + 1) * vdim].astype(
                    jnp.bfloat16
                )

    def score(head):
        return jnp.dot(q_ref[head], kt[head], preferred_element_type=jnp.float32)

    def weigh(head, scores, top):
        weights = jnp.exp2(scores - top).astype(jnp.bfloat16)
        return lax.dot_general(
            weights, vt[head], (((1,), (1,)), ((), ())), preferred_element_type=jnp.float32
        )

    def visit(pair):
        expand(pair)
        ahead = score(0)
        for head in range(heads):
            scores = ahead
            if head + 1 < heads:
                ahead = score(head + 1)
            old = run_max[head]
            top = jnp.maximum(old[:, :1], jnp.max(scores, axis=1, keepdims=True))
            wide_top = jnp.broadcast_to(top, (rows, lanes))
            run_max[head] = wide_top
            acc[head] = acc[head] * jnp.exp2(old - wide_top) + weigh(head, scores, top)

    kt[:, nope + rot :, :] = jnp.zeros((heads, lanes - nope - rot, wide), jnp.bfloat16)
    vt[:, vdim:, :] = jnp.ones((heads, lanes - vdim, wide), jnp.bfloat16)
    hand_over(0)
    relay(1)
    gathered(0)
    expand(last)
    key_pos = last * wide + lax.broadcasted_iota(jnp.int32, (rows, wide), 1)
    query_pos = me * rows + lax.broadcasted_iota(jnp.int32, (rows, wide), 0)
    hidden = key_pos > query_pos
    ahead = score(0)
    for head in range(heads):
        scores = jnp.where(hidden, far_below, ahead)
        if head + 1 < heads:
            ahead = score(head + 1)
        top = jnp.max(scores, axis=1, keepdims=True)
        run_max[head] = jnp.broadcast_to(top, (rows, lanes))
        acc[head] = weigh(head, scores, top)
    hand_over(1)
    relay(2)

    per_layer = PLANE // pairing
    first = layer * per_layer

    def near(step, carry):
        visit(last - 1 - step)
        return carry

    lax.fori_loop(0, last - first, near, 0)

    def far(step, carry):
        gathered_all(step)

        def one(turn, inner):
            @pl.when(turn == 1)
            def _():
                hand_over(step + 1)
                relay(step + 2)

            visit((layer - step) * per_layer + per_layer - 1 - turn)
            return inner

        lax.fori_loop(0, per_layer, one, 0)
        return carry

    def gathered_all(step):
        for d in range(PLANE):
            core_copy((layer - step) * PLANE + spot_at(d)).wait_recv()

    lax.fori_loop(1, layer + 1, far, 0)
    lane = lax.broadcasted_iota(jnp.int32, (rows, lanes), 1)
    for pair in range(heads // 2):
        halves = []
        for head in (2 * pair, 2 * pair + 1):
            total = acc[head]
            halves.append(total / pltpu.roll(total, vdim, axis=1))
        both = jnp.where(lane < vdim, halves[0], pltpu.roll(halves[1], vdim, axis=1))
        o_ref[:, pair * lanes : (pair + 1) * lanes] = both.astype(jnp.bfloat16)

    for d in range(1, layers):

        @pl.when(layer + d < layers)
        def _(d=d):
            column_copy(d).wait_send()

    def settle(step, carry):
        base = (layer - step) * PLANE
        for d in range(1, PLANE):
            plane_copy(own_ref.at[half], base + spot, d).wait_send()
            core_copy(base + spot_at(d)).wait_send()

        @pl.when(step > 0)
        def _():
            core_copy(base + spot).wait_send()

        return carry

    lax.fori_loop(0, layer + 1, settle, 0)


def attention(q_heads, packed, key_up_t, value_up_t):
    heads, rows, lanes = q_heads.shape
    blocks = lax.axis_size("sp")
    wide = 2 * rows
    layers = blocks // PLANE
    vmem = pl.BlockSpec(memory_space=pltpu.VMEM)
    dma = pltpu.SemaphoreType.DMA
    return pl.pallas_call(
        attention_kernel,
        out_shape=jax.ShapeDtypeStruct((rows, value_up_t.shape[0]), jnp.bfloat16),
        in_specs=[vmem] * 4,
        out_specs=vmem,
        scratch_shapes=[
            pltpu.VMEM((heads, lanes, wide), jnp.bfloat16),
            pltpu.VMEM((heads, lanes, wide), jnp.bfloat16),
            pltpu.VMEM((heads, rows, lanes), jnp.float32),
            pltpu.VMEM((heads, rows, lanes), jnp.float32),
            pltpu.VMEM((blocks,) + packed.shape, jnp.bfloat16),
            dma((max(layers - 1, 1),)),
            dma((layers, PLANE - 1)),
            dma((blocks,)),
            dma((blocks,)),
            dma((blocks,)),
        ],
        compiler_params=pltpu.CompilerParams(
            vmem_limit_bytes=56 << 20, collective_id=2, has_side_effects=True
        ),
        name="attention",
    )(q_heads, packed, key_up_t, value_up_t)


def gathered_kernel(q_ref, lat_ref, kup_ref, vup_ref, o_ref, kt, vt, run_max, acc):
    heads, rows, lanes = q_ref.shape
    blocks = lat_ref.shape[0]
    rank = kup_ref.shape[1]
    nope = kup_ref.shape[0] // heads
    vdim = vup_ref.shape[0] // heads
    rot = lat_ref.shape[1] - rank
    wide = kt.shape[2]
    group = wide // rows
    me = lax.axis_index("sp")
    last = me // group
    kt[:, nope + rot :, :] = jnp.zeros((heads, lanes - nope - rot, wide), jnp.bfloat16)
    vt[:, vdim:, :] = jnp.ones((heads, lanes - vdim, wide), jnp.bfloat16)

    def expand(block):
        for part in range(group):
            src = jnp.minimum(block * group + part, blocks - 1)
            lat = lat_ref[src, :rank, :]
            turned = lat_ref[src, rank:, :]
            cols = slice(part * rows, (part + 1) * rows)
            keys = jnp.dot(kup_ref[...], lat, preferred_element_type=jnp.float32)
            values = jnp.dot(vup_ref[...], lat, preferred_element_type=jnp.float32)
            for head in range(heads):
                kt[head, :nope, cols] = keys[head * nope : (head + 1) * nope].astype(jnp.bfloat16)
                kt[head, nope : nope + rot, cols] = turned
                vt[head, :vdim, cols] = values[head * vdim : (head + 1) * vdim].astype(
                    jnp.bfloat16
                )

    def weigh(head, scores, top):
        weights = jnp.exp2(scores - top).astype(jnp.bfloat16)
        return lax.dot_general(
            weights, vt[head], (((1,), (1,)), ((), ())), preferred_element_type=jnp.float32
        )

    expand(last)
    key_pos = last * wide + lax.broadcasted_iota(jnp.int32, (rows, wide), 1)
    query_pos = me * rows + lax.broadcasted_iota(jnp.int32, (rows, wide), 0)
    hidden = key_pos > query_pos
    for head in range(heads):
        scores = jnp.dot(q_ref[head], kt[head], preferred_element_type=jnp.float32)
        scores = jnp.where(hidden, far_below, scores)
        top = jnp.max(scores, axis=1, keepdims=True)
        run_max[head] = jnp.broadcast_to(top, (rows, lanes))
        acc[head] = weigh(head, scores, top)

    def visit(step, carry):
        expand(step)
        for head in range(heads):
            scores = jnp.dot(q_ref[head], kt[head], preferred_element_type=jnp.float32)
            old = run_max[head]
            top = jnp.maximum(old[:, :1], jnp.max(scores, axis=1, keepdims=True))
            wide_top = jnp.broadcast_to(top, (rows, lanes))
            run_max[head] = wide_top
            acc[head] = acc[head] * jnp.exp2(old - wide_top) + weigh(head, scores, top)
        return carry

    lax.fori_loop(0, last, visit, 0)
    lane = lax.broadcasted_iota(jnp.int32, (rows, lanes), 1)
    for pair in range(heads // 2):
        halves = []
        for head in (2 * pair, 2 * pair + 1):
            total = acc[head]
            halves.append(total / pltpu.roll(total, vdim, axis=1))
        both = jnp.where(lane < vdim, halves[0], pltpu.roll(halves[1], vdim, axis=1))
        o_ref[:, pair * lanes : (pair + 1) * lanes] = both.astype(jnp.bfloat16)


def gathered_attention(q_heads, lat_all, key_up_t, value_up_t):
    heads, rows, lanes = q_heads.shape
    blocks = lat_all.shape[0]
    wide = 2 * rows if blocks % 2 == 0 else rows
    vmem = pl.BlockSpec(memory_space=pltpu.VMEM)
    return pl.pallas_call(
        gathered_kernel,
        out_shape=jax.ShapeDtypeStruct((rows, value_up_t.shape[0]), jnp.bfloat16),
        in_specs=[vmem] * 4,
        out_specs=vmem,
        scratch_shapes=[
            pltpu.VMEM((heads, lanes, wide), jnp.bfloat16),
            pltpu.VMEM((heads, lanes, wide), jnp.bfloat16),
            pltpu.VMEM((heads, rows, lanes), jnp.float32),
            pltpu.VMEM((heads, rows, lanes), jnp.float32),
        ],
        compiler_params=pltpu.CompilerParams(vmem_limit_bytes=48 << 20),
        cost_estimate=pl.CostEstimate(
            flops=20_000_000_000, bytes_accessed=8 << 20, transcendentals=20_000_000
        ),
        name="gathered_attention",
    )(q_heads, lat_all, key_up_t, value_up_t)


def conv_kernel(gated_ref, rim_ref, taps_ref, out_ref, wide):
    rows, chans = gated_ref.shape
    rim = rim_ref.shape[0]
    taps = taps_ref.shape[0]
    chunk = 64
    for part in range(chans // 128):
        cols = slice(part * 128, (part + 1) * 128)
        wide[part, :rim, :] = rim_ref[:, cols].astype(jnp.float32)
        wide[part, rim:, :] = gated_ref[:, cols].astype(jnp.float32)
        coeff = taps_ref[:, cols]

        def band(step, carry):
            base = step * chunk
            total = jnp.zeros((chunk, 128), jnp.float32)
            for tap in range(taps):
                total = total + coeff[tap : tap + 1, :] * wide[
                    part, pl.ds(base + (rim - taps + 1 + tap), chunk), :
                ]
            out_ref[pl.ds(pl.multiple_of(base, chunk), chunk), cols] = total
            return carry

        lax.fori_loop(0, rows // chunk, band, 0)


def convolve(gated, rim, taps):
    rows, chans = gated.shape
    vmem = pl.BlockSpec(memory_space=pltpu.VMEM)
    return pl.pallas_call(
        conv_kernel,
        out_shape=jax.ShapeDtypeStruct((rows, chans), jnp.float32),
        in_specs=[vmem] * 3,
        out_specs=vmem,
        scratch_shapes=[pltpu.VMEM((chans // 128, rows + rim.shape[0], 128), jnp.float32)],
        cost_estimate=pl.CostEstimate(
            flops=2 * rows * chans * 31, bytes_accessed=2 << 20, transcendentals=0
        ),
        name="depthwise",
    )(gated, rim, taps)


def shards(
    tokens,
    input_gain,
    query_weight,
    query_rot_weight,
    kv_down,
    rot_down,
    kv_gain,
    key_up,
    value_up,
    conv_value_weight,
    conv_gate_weight,
    conv_taps,
    conv_ln_gain,
    conv_ln_bias,
    att_out_gain,
    conv_out_gain,
    att_out_weight,
    conv_out_weight,
):
    tok_rows = tokens.shape[0]
    heads_here = key_up.shape[1] // NOPE_DIM
    chan_here = conv_taps.shape[1]
    weight_list = (
        query_weight,
        query_rot_weight,
        kv_down,
        rot_down,
        conv_value_weight,
        conv_gate_weight,
    )
    paired = lax.axis_size("tp") == 2 and lax.axis_size("sp") % PLANE == 0
    if paired:
        scaled, row_scale = exchange_tokens(tokens, input_gain[None, :])
    else:
        whole_rows = lax.all_gather(tokens, "tp", axis=1, tiled=True).astype(jnp.float32)
        scaled = (whole_rows * input_gain[None, :]).astype(jnp.bfloat16)
        row_scale = lax.rsqrt(
            jnp.mean(whole_rows * whole_rows, axis=1, keepdims=True) + norm_eps
        )

    def add_product(weight):
        return jnp.dot(scaled, weight, preferred_element_type=jnp.float32)

    summed = tuple((add_product(weight) for weight in weight_list))
    q_acc, qrot_acc, latent_raw, rot_acc, value_acc, gate_acc = summed
    positions = lax.axis_index("sp") * tok_rows + jnp.arange(tok_rows, dtype=jnp.int32)
    cos_table, sine_table = rotary_tables(positions, ROT_DIM // 2)
    fold = math.log2(math.e) / math.sqrt(NOPE_DIM + ROT_DIM)
    query_scale = row_scale * fold
    plain_q = (q_acc * query_scale).reshape(tok_rows, heads_here, NOPE_DIM)
    turned_q = rotate_half(
        (qrot_acc * query_scale).reshape(tok_rows, heads_here, ROT_DIM),
        cos_table[:, None, :],
        sine_table[:, None, :],
    )
    blank = jnp.zeros((tok_rows, heads_here, 128 - NOPE_DIM - ROT_DIM), jnp.float32)
    q_heads = jnp.transpose(
        jnp.concatenate([plain_q, turned_q, blank], axis=2).astype(jnp.bfloat16), (1, 0, 2)
    )
    latent = (
        latent_raw
        * lax.rsqrt(jnp.mean(latent_raw * latent_raw, axis=1, keepdims=True) + norm_eps)
        * kv_gain[None, :]
    ).astype(jnp.bfloat16)
    key_rot = rotate_half(rot_acc * row_scale, cos_table, sine_table).astype(jnp.bfloat16)
    gated_input = (value_acc * row_scale * jax.nn.sigmoid(gate_acc * row_scale)).astype(
        jnp.bfloat16
    )
    packed = jnp.concatenate([latent.T, key_rot.T], axis=0)
    rim_rows = shifted(gated_input[tok_rows - (KERNEL + 1) :], "sp", 1)
    conv_out = convolve(gated_input, rim_rows, conv_taps)
    moment_one, moment_two = lax.psum(
        (jnp.sum(conv_out, axis=1), jnp.sum(conv_out * conv_out, axis=1)), "tp"
    )
    mean_val = moment_one / CONV_CH
    spread = moment_two / CONV_CH - mean_val * mean_val
    normed = (conv_out - mean_val[:, None]) * lax.rsqrt(spread + norm_eps)[:, None]
    swished = jax.nn.silu(normed * conv_ln_gain[None, :] + conv_ln_bias[None, :])
    if paired:
        attended = attention(q_heads, packed, key_up.T, value_up.T)
        return merge(
            attended,
            swished,
            att_out_gain[None, :],
            conv_out_gain[None, :],
            att_out_weight,
            conv_out_weight,
        )
    lat_all = lax.all_gather(packed, "sp", axis=0)
    attended = gathered_attention(q_heads, lat_all, key_up.T, value_up.T).astype(jnp.float32)
    att_sq, conv_sq = lax.psum(
        (
            jnp.sum(attended * attended, axis=1, keepdims=True),
            jnp.sum(swished * swished, axis=1, keepdims=True),
        ),
        "tp",
    )
    att_mixed = (
        attended * lax.rsqrt(att_sq / ATT_WIDTH + norm_eps) * att_out_gain[None, :]
    ).astype(jnp.bfloat16)
    conv_mixed = (
        swished * lax.rsqrt(conv_sq / CONV_CH + norm_eps) * conv_out_gain[None, :]
    ).astype(jnp.bfloat16)
    share = (
        jnp.dot(att_mixed, att_out_weight, preferred_element_type=jnp.float32)
        + jnp.dot(conv_mixed, conv_out_weight, preferred_element_type=jnp.float32)
    ).astype(jnp.bfloat16)
    return lax.psum_scatter(share, "tp", scatter_dimension=1, tiled=True)


def solution(mesh):
    return jax.shard_map(
        shards,
        mesh=mesh,
        in_specs=(
            P("sp", "tp"),
            P(),
            P(None, "tp"),
            P(None, "tp"),
            P(),
            P(),
            P(),
            P(None, "tp"),
            P(None, "tp"),
            P(None, "tp"),
            P(None, "tp"),
            P(None, "tp"),
            P("tp"),
            P("tp"),
            P("tp"),
            P("tp"),
            P("tp", None),
            P("tp", None),
        ),
        out_specs=P("sp", "tp"),
        check_vma=False,
    )
```

```python
import math

import jax
import jax.numpy as jnp
from jax import lax
from jax.experimental import pallas as pl
from jax.experimental.pallas import tpu as pltpu
from jax.sharding import PartitionSpec as P

D_MODEL = 2048
NOPE_DIM = 64
ROT_DIM = 32
VALUE_DIM = 64
CONV_CH = 1024
KERNEL = 31
ATT_WIDTH = 1024


norm_eps = 1e-06
far_below = -1e30
rope_base = 10000.0


def shifted(block, axis, distance):
    devices = range(lax.axis_size(axis))
    route = [(i - distance, i) for i in devices if i - distance in devices]
    return lax.ppermute(block, axis, route)


def rotary_tables(positions, half_dim):
    frequency = rope_base ** (-jnp.arange(half_dim, dtype=jnp.float32) / half_dim)
    angles = positions.astype(jnp.float32)[:, None] * frequency[None, :]
    return (jnp.cos(angles), jnp.sin(angles))


def rotate_half(values, cos_table, sine_table):
    half_dim = cos_table.shape[-1]
    front_half = values[..., :half_dim]
    back_half = values[..., half_dim:]
    return jnp.concatenate(
        [
            front_half * cos_table - back_half * sine_table,
            back_half * cos_table + front_half * sine_table,
        ],
        axis=-1,
    )


MESH = pl.DeviceIdType.MESH


def push(src, dst, send, recv, target):
    return pltpu.make_async_remote_copy(
        src_ref=src,
        dst_ref=dst,
        send_sem=send,
        recv_sem=recv,
        device_id=target,
        device_id_type=MESH,
    )


def greet(targets):
    barrier = pltpu.get_barrier_semaphore()
    for target in targets:
        pl.semaphore_signal(barrier, inc=1, device_id=target, device_id_type=MESH)
    pl.semaphore_wait(barrier, len(targets))


def other_core():
    return {"sp": lax.axis_index("sp"), "tp": 1 - lax.axis_index("tp")}


def front_kernel(
    tok_ref, gain_ref, kv_gain_ref, cos_ref, sin_ref, taps_ref, ln_gain_ref, ln_bias_ref,
    qw_hbm, qrw_hbm, kvd_hbm, rotw_hbm, cvw_hbm, cgw_hbm,
    q_ref, packed_ref, swish_ref,
    qw, qrw, kvd, rotw, cvw, cgw, scaled, landed, narrow, gated, rim, wide, conv,
    sq_mine, sq_other, w_sem, tok_send, tok_recv, rim_send, rim_recv, sq_send, sq_recv,
):
    mine = lax.axis_index("tp")
    seat = lax.axis_index("sp")
    seats = lax.axis_size("sp")
    rows, width = tok_ref.shape
    heads, _, lanes = q_ref.shape
    loads = [
        pltpu.make_async_copy(src, dst, w_sem.at[index])
        for index, (src, dst) in enumerate(
            (
                (kvd_hbm, kvd), (rotw_hbm, rotw), (cvw_hbm, cvw),
                (cgw_hbm, cgw), (qw_hbm, qw), (qrw_hbm, qrw),
            )
        )
    ]
    for load in loads:
        load.start()
    ahead = {"sp": (seat + 1) % seats, "tp": mine}
    behind = {"sp": (seat + seats - 1) % seats, "tp": mine}
    greet([other_core(), ahead, behind])
    copy = push(tok_ref, landed, tok_send, tok_recv, other_core())
    copy.start()

    def place(block, index):
        cols = pl.ds(pl.multiple_of(index * width, 128), width)
        full = block[...].astype(jnp.float32)
        scaled[:, cols] = (full * gain_ref[:, cols]).astype(jnp.bfloat16)
        return jnp.sum(full * full, axis=1, keepdims=True)

    squares = place(tok_ref, mine)
    copy.wait()
    squares = squares + place(landed, 1 - mine)
    row_scale = lax.rsqrt(squares / (2 * width) + norm_eps)

    def project(weight):
        return jnp.dot(scaled[...], weight[...], preferred_element_type=jnp.float32)

    loads[2].wait()
    loads[3].wait()
    gate = project(cgw) * row_scale
    gated[...] = (project(cvw) * row_scale * jax.nn.sigmoid(gate)).astype(jnp.bfloat16)
    edge = rim.shape[0]
    rim_copy = push(gated.at[pl.ds(rows - edge, edge)], rim, rim_send, rim_recv, ahead)

    @pl.when(seat < seats - 1)
    def _():
        rim_copy.start()

    loads[0].wait()
    loads[1].wait()
    raw = project(kvd)
    rank = raw.shape[1]
    latent = (
        raw
        * lax.rsqrt(jnp.mean(raw * raw, axis=1, keepdims=True) + norm_eps)
        * kv_gain_ref[...]
    )
    packed_ref[:rank, :] = latent.T.astype(jnp.bfloat16)
    cos_table = cos_ref[...]
    sin_table = sin_ref[...]
    turn = cos_table.shape[0]

    def rotate(block):
        front = block[:turn]
        back = block[turn : 2 * turn]
        return jnp.concatenate(
            [front * cos_table - back * sin_table, back * cos_table + front * sin_table], axis=0
        )

    narrow[...] = jnp.zeros(narrow.shape, jnp.float32)
    narrow[:, : 2 * turn] = project(rotw) * row_scale
    packed_ref[rank:, :] = rotate(narrow[...].T).astype(jnp.bfloat16)
    loads[4].wait()
    loads[5].wait()
    query_scale = row_scale * (math.log2(math.e) / math.sqrt(NOPE_DIM + ROT_DIM))
    plain = (project(qw) * query_scale).T
    turned = (project(qrw) * query_scale).T
    blank = jnp.zeros((lanes - NOPE_DIM - ROT_DIM, rows), jnp.float32)
    for head in range(heads):
        column = jnp.concatenate(
            [
                plain[head * NOPE_DIM : (head + 1) * NOPE_DIM],
                rotate(turned[head * ROT_DIM : (head + 1) * ROT_DIM]),
                blank,
            ],
            axis=0,
        )
        q_ref[head] = column.T.astype(jnp.bfloat16)

    @pl.when(seat > 0)
    def _():
        rim_copy.wait_recv()

    @pl.when(seat == 0)
    def _():
        rim[...] = jnp.zeros(rim.shape, jnp.bfloat16)

    taps = taps_ref.shape[0]
    chunk = 64
    for part in range(conv.shape[1] // 128):
        cols = slice(part * 128, (part + 1) * 128)
        wide[part, :edge, :] = rim[:, cols].astype(jnp.float32)
        wide[part, edge:, :] = gated[:, cols].astype(jnp.float32)
        coeff = taps_ref[:, cols]

        def band(step, carry, part=part, cols=cols, coeff=coeff):
            base = step * chunk
            total = jnp.zeros((chunk, 128), jnp.float32)
            for tap in range(taps):
                total = total + coeff[tap : tap + 1, :] * wide[
                    part, pl.ds(base + (edge - taps + 1 + tap), chunk), :
                ]
            conv[pl.ds(pl.multiple_of(base, chunk), chunk), cols] = total
            return carry

        lax.fori_loop(0, rows // chunk, band, 0)

    values = conv[...]
    for slot, total in enumerate((values, values * values)):
        sq_mine[:, slot * 128 : (slot + 1) * 128] = jnp.broadcast_to(
            jnp.sum(total, axis=1, keepdims=True), (rows, 128)
        )
    sums = push(sq_mine, sq_other, sq_send, sq_recv, other_core())
    sums.start()
    sums.wait()
    moments = (sq_mine[...] + sq_other[...]) / CONV_CH
    mean_val = moments[:, :1]
    spread = moments[:, 128:129] - mean_val * mean_val
    normed = (values - mean_val) * lax.rsqrt(spread + norm_eps)
    swish_ref[...] = jax.nn.silu(normed * ln_gain_ref[...] + ln_bias_ref[...])

    @pl.when(seat < seats - 1)
    def _():
        rim_copy.wait_send()


def front(tokens, gain, kv_gain, cos_t, sin_t, taps, ln_gain, ln_bias, weights):
    rows, width = tokens.shape
    chans = taps.shape[1]
    heads = weights[0].shape[1] // NOPE_DIM
    rank = weights[2].shape[1]
    vmem = pl.BlockSpec(memory_space=pltpu.VMEM)
    anywhere = pl.BlockSpec(memory_space=pl.ANY)
    dma = pltpu.SemaphoreType.DMA
    edge = 32
    return pl.pallas_call(
        front_kernel,
        out_shape=(
            jax.ShapeDtypeStruct((heads, rows, 128), jnp.bfloat16),
            jax.ShapeDtypeStruct((rank + ROT_DIM, rows), jnp.bfloat16),
            jax.ShapeDtypeStruct((rows, chans), jnp.float32),
        ),
        in_specs=[vmem] * 8 + [anywhere] * 6,
        out_specs=(vmem,) * 3,
        scratch_shapes=[pltpu.VMEM(weight.shape, jnp.bfloat16) for weight in weights]
        + [
            pltpu.VMEM((rows, 2 * width), jnp.bfloat16),
            pltpu.VMEM((rows, width), jnp.bfloat16),
            pltpu.VMEM((rows, 128), jnp.float32),
            pltpu.VMEM((rows, chans), jnp.bfloat16),
            pltpu.VMEM((edge, chans), jnp.bfloat16),
            pltpu.VMEM((chans // 128, rows + edge, 128), jnp.float32),
            pltpu.VMEM((rows, chans), jnp.float32),
            pltpu.VMEM((rows, 256), jnp.float32),
            pltpu.VMEM((rows, 256), jnp.float32),
            dma((6,)),
        ]
        + [dma] * 6,
        compiler_params=pltpu.CompilerParams(
            vmem_limit_bytes=40 << 20, collective_id=0, has_side_effects=True
        ),
        name="front",
    )(tokens, gain, kv_gain, cos_t, sin_t, taps, ln_gain, ln_bias, *weights)


def output_kernel(
    att_ref, swish_ref, att_gain, conv_gain, att_hbm, conv_hbm, out_ref,
    att_w, conv_w, sq_mine, sq_other, part, landed, w_sem, sq_send, sq_recv, send, recv,
):
    loads = [
        pltpu.make_async_copy(att_hbm, att_w, w_sem.at[0]),
        pltpu.make_async_copy(conv_hbm, conv_w, w_sem.at[1]),
    ]
    for load in loads:
        load.start()
    mine = lax.axis_index("tp")
    rows, width = out_ref.shape
    lanes = sq_mine.shape[1] // 2
    attended = att_ref[...].astype(jnp.float32)
    swished = swish_ref[...]
    for slot, value in enumerate((attended, swished)):
        total = jnp.sum(value * value, axis=1, keepdims=True)
        sq_mine[:, slot * lanes : (slot + 1) * lanes] = jnp.broadcast_to(total, (rows, lanes))
    greet([other_core()])
    sums = push(sq_mine, sq_other, sq_send, sq_recv, other_core())
    sums.start()
    sums.wait()
    sq = sq_mine[...] + sq_other[...]
    att_scale = lax.rsqrt(sq[:, :1] / ATT_WIDTH + norm_eps)
    conv_scale = lax.rsqrt(sq[:, lanes : lanes + 1] / CONV_CH + norm_eps)
    att_mixed = (attended * att_scale * att_gain[...]).astype(jnp.bfloat16)
    conv_mixed = (swished * conv_scale * conv_gain[...]).astype(jnp.bfloat16)
    piece = part.shape[2]
    pieces = part.shape[0]

    def product(owner, index):
        cols = pl.ds(pl.multiple_of(owner * width + index * piece, 128), piece)
        return (
            jnp.dot(att_mixed, att_w[:, cols], preferred_element_type=jnp.float32)
            + jnp.dot(conv_mixed, conv_w[:, cols], preferred_element_type=jnp.float32)
        ).astype(jnp.bfloat16)

    for load in loads:
        load.wait()
    copies = []
    for index in range(pieces):
        part[index] = product(1 - mine, index)
        copy = push(
            part.at[index], landed.at[index], send.at[index], recv.at[index], other_core()
        )
        copy.start()
        copies.append(copy)
    for index in range(pieces):
        own = product(mine, index).astype(jnp.float32)
        copies[index].wait()
        out_ref[:, index * piece : (index + 1) * piece] = (
            own + landed[index].astype(jnp.float32)
        ).astype(jnp.bfloat16)


def merge(attended, swished, att_gain, conv_gain, att_w, conv_w):
    rows = attended.shape[0]
    width = att_w.shape[1] // 2
    pieces = 4
    vmem = pl.BlockSpec(memory_space=pltpu.VMEM)
    return pl.pallas_call(
        output_kernel,
        out_shape=jax.ShapeDtypeStruct((rows, width), jnp.bfloat16),
        in_specs=[vmem] * 4 + [pl.BlockSpec(memory_space=pl.ANY)] * 2,
        out_specs=vmem,
        scratch_shapes=[
            pltpu.VMEM(att_w.shape, jnp.bfloat16),
            pltpu.VMEM(conv_w.shape, jnp.bfloat16),
            pltpu.VMEM((rows, 256), jnp.float32),
            pltpu.VMEM((rows, 256), jnp.float32),
            pltpu.VMEM((pieces, rows, width // pieces), jnp.bfloat16),
            pltpu.VMEM((pieces, rows, width // pieces), jnp.bfloat16),
            pltpu.SemaphoreType.DMA((2,)),
            pltpu.SemaphoreType.DMA,
            pltpu.SemaphoreType.DMA,
            pltpu.SemaphoreType.DMA((pieces,)),
            pltpu.SemaphoreType.DMA((pieces,)),
        ],
        compiler_params=pltpu.CompilerParams(collective_id=1, has_side_effects=True),
        name="output_merge",
    )(attended, swished, att_gain, conv_gain, att_w, conv_w)


PLANE = 4


def attention_kernel(
    q_ref, own_ref, kup_ref, vup_ref, o_ref, kt, vt, run_max, acc, lat_ref,
    col_send, plane_send, core_send, link_recv, core_recv,
):
    heads, rows, lanes = q_ref.shape
    blocks = lat_ref.shape[0]
    rank = kup_ref.shape[1]
    nope = kup_ref.shape[0] // heads
    vdim = vup_ref.shape[0] // heads
    rot = lat_ref.shape[1] - rank
    wide = kt.shape[2]
    pairing = wide // rows
    me = lax.axis_index("sp")
    core = lax.axis_index("tp")
    layers = blocks // PLANE
    layer = me // PLANE
    spot = me % PLANE
    last = me // pairing
    height = lat_ref.shape[1] // 2
    half = pl.ds(pl.multiple_of(core * height, 16), height)

    def spot_at(distance):
        return (spot + distance) % PLANE

    def at(layer_id, spot_id):
        return {"sp": layer_id * PLANE + spot_id, "tp": core}

    greet(
        [at((layer + d) % layers, spot) for d in range(1, layers)]
        + [at(layer, spot_at(d)) for d in range(1, PLANE)]
        + [other_core()]
    )

    def column_copy(distance):
        return push(
            own_ref.at[half],
            lat_ref.at[me, half],
            col_send.at[distance - 1],
            link_recv.at[me],
            at(jnp.minimum(layer + distance, layers - 1), spot),
        )

    def plane_copy(source, block, distance):
        return push(
            source,
            lat_ref.at[block, half],
            plane_send.at[block // PLANE, distance - 1],
            link_recv.at[block],
            at(layer, spot_at(distance)),
        )

    def core_copy(block):
        spread = lat_ref.at[block, half]
        return push(spread, spread, core_send.at[block], core_recv.at[block], other_core())

    for d in range(1, PLANE):
        plane_copy(own_ref.at[half], me, d).start()
    for d in range(1, layers):

        @pl.when(layer + d < layers)
        def _(d=d):
            column_copy(d).start()

    lat_ref[me] = own_ref[...]

    def relay(step):
        @pl.when(step <= layer)
        def _():
            block = (layer - step) * PLANE + spot
            landed(block)
            for d in range(1, PLANE):
                plane_copy(lat_ref.at[block, half], block, d).start()
            core_copy(block).start()

    def hand_over(step):
        @pl.when(step <= layer)
        def _():
            for d in range(1, PLANE):
                block = (layer - step) * PLANE + spot_at(d)
                landed(block)
                core_copy(block).start()

    def landed(block):
        spread = lat_ref.at[block, half]
        push(spread, spread, core_send.at[block], link_recv.at[block], other_core()).wait_recv()

    def gathered(step):
        for d in range(1, PLANE):
            core_copy((layer - step) * PLANE + spot_at(d)).wait_recv()

    def expand(pair):
        for part in range(pairing):
            src = pair * pairing + part
            lat = lat_ref[src, :rank, :]
            turned = lat_ref[src, rank:, :]
            cols = slice(part * rows, (part + 1) * rows)
            keys = jnp.dot(kup_ref[...], lat, preferred_element_type=jnp.float32)
            values = jnp.dot(vup_ref[...], lat, preferred_element_type=jnp.float32)
            for head in range(heads):
                kt[head, :nope, cols] = keys[head * nope : (head + 1) * nope].astype(jnp.bfloat16)
                kt[head, nope : nope + rot, cols] = turned
                vt[head, :vdim, cols] = values[head * vdim : (head + 1) * vdim].astype(
                    jnp.bfloat16
                )

    def score(head):
        return jnp.dot(q_ref[head], kt[head], preferred_element_type=jnp.float32)

    def weigh(head, scores, top):
        weights = jnp.exp2(scores - top).astype(jnp.bfloat16)
        return lax.dot_general(
            weights, vt[head], (((1,), (1,)), ((), ())), preferred_element_type=jnp.float32
        )

    def visit(pair):
        expand(pair)
        ahead = score(0)
        for head in range(heads):
            scores = ahead
            if head + 1 < heads:
                ahead = score(head + 1)
            old = run_max[head]
            top = jnp.maximum(old[:, :1], jnp.max(scores, axis=1, keepdims=True))
            wide_top = jnp.broadcast_to(top, (rows, lanes))
            run_max[head] = wide_top
            acc[head] = acc[head] * jnp.exp2(old - wide_top) + weigh(head, scores, top)

    kt[:, nope + rot :, :] = jnp.zeros((heads, lanes - nope - rot, wide), jnp.bfloat16)
    vt[:, vdim:, :] = jnp.ones((heads, lanes - vdim, wide), jnp.bfloat16)
    hand_over(0)
    relay(1)
    gathered(0)
    expand(last)
    key_pos = last * wide + lax.broadcasted_iota(jnp.int32, (rows, wide), 1)
    query_pos = me * rows + lax.broadcasted_iota(jnp.int32, (rows, wide), 0)
    hidden = key_pos > query_pos
    ahead = score(0)
    for head in range(heads):
        scores = jnp.where(hidden, far_below, ahead)
        if head + 1 < heads:
            ahead = score(head + 1)
        top = jnp.max(scores, axis=1, keepdims=True)
        run_max[head] = jnp.broadcast_to(top, (rows, lanes))
        acc[head] = weigh(head, scores, top)
    hand_over(1)
    relay(2)

    per_layer = PLANE // pairing
    first = layer * per_layer

    def near(step, carry):
        visit(last - 1 - step)
        return carry

    lax.fori_loop(0, last - first, near, 0)

    def far(step, carry):
        gathered_all(step)

        def one(turn, inner):
            @pl.when(turn == 1)
            def _():
                hand_over(step + 1)
                relay(step + 2)

            visit((layer - step) * per_layer + per_layer - 1 - turn)
            return inner

        lax.fori_loop(0, per_layer, one, 0)
        return carry

    def gathered_all(step):
        for d in range(PLANE):
            core_copy((layer - step) * PLANE + spot_at(d)).wait_recv()

    lax.fori_loop(1, layer + 1, far, 0)
    lane = lax.broadcasted_iota(jnp.int32, (rows, lanes), 1)
    for pair in range(heads // 2):
        halves = []
        for head in (2 * pair, 2 * pair + 1):
            total = acc[head]
            halves.append(total / pltpu.roll(total, vdim, axis=1))
        both = jnp.where(lane < vdim, halves[0], pltpu.roll(halves[1], vdim, axis=1))
        o_ref[:, pair * lanes : (pair + 1) * lanes] = both.astype(jnp.bfloat16)

    for d in range(1, layers):

        @pl.when(layer + d < layers)
        def _(d=d):
            column_copy(d).wait_send()

    def settle(step, carry):
        base = (layer - step) * PLANE
        for d in range(1, PLANE):
            plane_copy(own_ref.at[half], base + spot, d).wait_send()
            core_copy(base + spot_at(d)).wait_send()

        @pl.when(step > 0)
        def _():
            core_copy(base + spot).wait_send()

        return carry

    lax.fori_loop(0, layer + 1, settle, 0)


def attention(q_heads, packed, key_up_t, value_up_t):
    heads, rows, lanes = q_heads.shape
    blocks = lax.axis_size("sp")
    wide = 2 * rows
    layers = blocks // PLANE
    vmem = pl.BlockSpec(memory_space=pltpu.VMEM)
    dma = pltpu.SemaphoreType.DMA
    return pl.pallas_call(
        attention_kernel,
        out_shape=jax.ShapeDtypeStruct((rows, value_up_t.shape[0]), jnp.bfloat16),
        in_specs=[vmem] * 4,
        out_specs=vmem,
        scratch_shapes=[
            pltpu.VMEM((heads, lanes, wide), jnp.bfloat16),
            pltpu.VMEM((heads, lanes, wide), jnp.bfloat16),
            pltpu.VMEM((heads, rows, lanes), jnp.float32),
            pltpu.VMEM((heads, rows, lanes), jnp.float32),
            pltpu.VMEM((blocks,) + packed.shape, jnp.bfloat16),
            dma((max(layers - 1, 1),)),
            dma((layers, PLANE - 1)),
            dma((blocks,)),
            dma((blocks,)),
            dma((blocks,)),
        ],
        compiler_params=pltpu.CompilerParams(
            vmem_limit_bytes=24 << 20, collective_id=2, has_side_effects=True
        ),
        name="attention",
    )(q_heads, packed, key_up_t, value_up_t)


def gathered_kernel(q_ref, lat_ref, kup_ref, vup_ref, o_ref, kt, vt, run_max, acc):
    heads, rows, lanes = q_ref.shape
    blocks = lat_ref.shape[0]
    rank = kup_ref.shape[1]
    nope = kup_ref.shape[0] // heads
    vdim = vup_ref.shape[0] // heads
    rot = lat_ref.shape[1] - rank
    wide = kt.shape[2]
    group = wide // rows
    me = lax.axis_index("sp")
    last = me // group
    kt[:, nope + rot :, :] = jnp.zeros((heads, lanes - nope - rot, wide), jnp.bfloat16)
    vt[:, vdim:, :] = jnp.ones((heads, lanes - vdim, wide), jnp.bfloat16)

    def expand(block):
        for part in range(group):
            src = jnp.minimum(block * group + part, blocks - 1)
            lat = lat_ref[src, :rank, :]
            turned = lat_ref[src, rank:, :]
            cols = slice(part * rows, (part + 1) * rows)
            keys = jnp.dot(kup_ref[...], lat, preferred_element_type=jnp.float32)
            values = jnp.dot(vup_ref[...], lat, preferred_element_type=jnp.float32)
            for head in range(heads):
                kt[head, :nope, cols] = keys[head * nope : (head + 1) * nope].astype(jnp.bfloat16)
                kt[head, nope : nope + rot, cols] = turned
                vt[head, :vdim, cols] = values[head * vdim : (head + 1) * vdim].astype(
                    jnp.bfloat16
                )

    def weigh(head, scores, top):
        weights = jnp.exp2(scores - top).astype(jnp.bfloat16)
        return lax.dot_general(
            weights, vt[head], (((1,), (1,)), ((), ())), preferred_element_type=jnp.float32
        )

    expand(last)
    key_pos = last * wide + lax.broadcasted_iota(jnp.int32, (rows, wide), 1)
    query_pos = me * rows + lax.broadcasted_iota(jnp.int32, (rows, wide), 0)
    hidden = key_pos > query_pos
    for head in range(heads):
        scores = jnp.dot(q_ref[head], kt[head], preferred_element_type=jnp.float32)
        scores = jnp.where(hidden, far_below, scores)
        top = jnp.max(scores, axis=1, keepdims=True)
        run_max[head] = jnp.broadcast_to(top, (rows, lanes))
        acc[head] = weigh(head, scores, top)

    def visit(step, carry):
        expand(step)
        for head in range(heads):
            scores = jnp.dot(q_ref[head], kt[head], preferred_element_type=jnp.float32)
            old = run_max[head]
            top = jnp.maximum(old[:, :1], jnp.max(scores, axis=1, keepdims=True))
            wide_top = jnp.broadcast_to(top, (rows, lanes))
            run_max[head] = wide_top
            acc[head] = acc[head] * jnp.exp2(old - wide_top) + weigh(head, scores, top)
        return carry

    lax.fori_loop(0, last, visit, 0)
    lane = lax.broadcasted_iota(jnp.int32, (rows, lanes), 1)
    for pair in range(heads // 2):
        halves = []
        for head in (2 * pair, 2 * pair + 1):
            total = acc[head]
            halves.append(total / pltpu.roll(total, vdim, axis=1))
        both = jnp.where(lane < vdim, halves[0], pltpu.roll(halves[1], vdim, axis=1))
        o_ref[:, pair * lanes : (pair + 1) * lanes] = both.astype(jnp.bfloat16)


def gathered_attention(q_heads, lat_all, key_up_t, value_up_t):
    heads, rows, lanes = q_heads.shape
    blocks = lat_all.shape[0]
    wide = 2 * rows if blocks % 2 == 0 else rows
    vmem = pl.BlockSpec(memory_space=pltpu.VMEM)
    return pl.pallas_call(
        gathered_kernel,
        out_shape=jax.ShapeDtypeStruct((rows, value_up_t.shape[0]), jnp.bfloat16),
        in_specs=[vmem] * 4,
        out_specs=vmem,
        scratch_shapes=[
            pltpu.VMEM((heads, lanes, wide), jnp.bfloat16),
            pltpu.VMEM((heads, lanes, wide), jnp.bfloat16),
            pltpu.VMEM((heads, rows, lanes), jnp.float32),
            pltpu.VMEM((heads, rows, lanes), jnp.float32),
        ],
        compiler_params=pltpu.CompilerParams(vmem_limit_bytes=48 << 20),
        cost_estimate=pl.CostEstimate(
            flops=20_000_000_000, bytes_accessed=8 << 20, transcendentals=20_000_000
        ),
        name="gathered_attention",
    )(q_heads, lat_all, key_up_t, value_up_t)


def conv_kernel(gated_ref, rim_ref, taps_ref, out_ref, wide):
    rows, chans = gated_ref.shape
    rim = rim_ref.shape[0]
    taps = taps_ref.shape[0]
    chunk = 64
    for part in range(chans // 128):
        cols = slice(part * 128, (part + 1) * 128)
        wide[part, :rim, :] = rim_ref[:, cols].astype(jnp.float32)
        wide[part, rim:, :] = gated_ref[:, cols].astype(jnp.float32)
        coeff = taps_ref[:, cols]

        def band(step, carry):
            base = step * chunk
            total = jnp.zeros((chunk, 128), jnp.float32)
            for tap in range(taps):
                total = total + coeff[tap : tap + 1, :] * wide[
                    part, pl.ds(base + (rim - taps + 1 + tap), chunk), :
                ]
            out_ref[pl.ds(pl.multiple_of(base, chunk), chunk), cols] = total
            return carry

        lax.fori_loop(0, rows // chunk, band, 0)


def convolve(gated, rim, taps):
    rows, chans = gated.shape
    vmem = pl.BlockSpec(memory_space=pltpu.VMEM)
    return pl.pallas_call(
        conv_kernel,
        out_shape=jax.ShapeDtypeStruct((rows, chans), jnp.float32),
        in_specs=[vmem] * 3,
        out_specs=vmem,
        scratch_shapes=[pltpu.VMEM((chans // 128, rows + rim.shape[0], 128), jnp.float32)],
        cost_estimate=pl.CostEstimate(
            flops=2 * rows * chans * 31, bytes_accessed=2 << 20, transcendentals=0
        ),
        name="depthwise",
    )(gated, rim, taps)


def shards(
    tokens,
    input_gain,
    query_weight,
    query_rot_weight,
    kv_down,
    rot_down,
    kv_gain,
    key_up,
    value_up,
    conv_value_weight,
    conv_gate_weight,
    conv_taps,
    conv_ln_gain,
    conv_ln_bias,
    att_out_gain,
    conv_out_gain,
    att_out_weight,
    conv_out_weight,
):
    tok_rows = tokens.shape[0]
    heads_here = key_up.shape[1] // NOPE_DIM
    chan_here = conv_taps.shape[1]
    weight_list = (
        query_weight,
        query_rot_weight,
        kv_down,
        rot_down,
        conv_value_weight,
        conv_gate_weight,
    )
    if lax.axis_size("tp") == 2 and lax.axis_size("sp") % PLANE == 0:
        positions = lax.axis_index("sp") * tok_rows + jnp.arange(tok_rows, dtype=jnp.int32)
        cos_table, sine_table = rotary_tables(positions, ROT_DIM // 2)
        q_heads, packed, swished = front(
            tokens,
            input_gain[None, :],
            kv_gain[None, :],
            cos_table.T,
            sine_table.T,
            conv_taps,
            conv_ln_gain[None, :],
            conv_ln_bias[None, :],
            weight_list,
        )
        attended = attention(q_heads, packed, key_up.T, value_up.T)
        return merge(
            attended,
            swished,
            att_out_gain[None, :],
            conv_out_gain[None, :],
            att_out_weight,
            conv_out_weight,
        )
    whole_rows = lax.all_gather(tokens, "tp", axis=1, tiled=True).astype(jnp.float32)
    scaled = (whole_rows * input_gain[None, :]).astype(jnp.bfloat16)
    row_scale = lax.rsqrt(jnp.mean(whole_rows * whole_rows, axis=1, keepdims=True) + norm_eps)

    def add_product(weight):
        return jnp.dot(scaled, weight, preferred_element_type=jnp.float32)

    summed = tuple((add_product(weight) for weight in weight_list))
    q_acc, qrot_acc, latent_raw, rot_acc, value_acc, gate_acc = summed
    positions = lax.axis_index("sp") * tok_rows + jnp.arange(tok_rows, dtype=jnp.int32)
    cos_table, sine_table = rotary_tables(positions, ROT_DIM // 2)
    fold = math.log2(math.e) / math.sqrt(NOPE_DIM + ROT_DIM)
    query_scale = row_scale * fold
    plain_q = (q_acc * query_scale).reshape(tok_rows, heads_here, NOPE_DIM)
    turned_q = rotate_half(
        (qrot_acc * query_scale).reshape(tok_rows, heads_here, ROT_DIM),
        cos_table[:, None, :],
        sine_table[:, None, :],
    )
    blank = jnp.zeros((tok_rows, heads_here, 128 - NOPE_DIM - ROT_DIM), jnp.float32)
    q_heads = jnp.transpose(
        jnp.concatenate([plain_q, turned_q, blank], axis=2).astype(jnp.bfloat16), (1, 0, 2)
    )
    latent = (
        latent_raw
        * lax.rsqrt(jnp.mean(latent_raw * latent_raw, axis=1, keepdims=True) + norm_eps)
        * kv_gain[None, :]
    ).astype(jnp.bfloat16)
    key_rot = rotate_half(rot_acc * row_scale, cos_table, sine_table).astype(jnp.bfloat16)
    gated_input = (value_acc * row_scale * jax.nn.sigmoid(gate_acc * row_scale)).astype(
        jnp.bfloat16
    )
    packed = jnp.concatenate([latent.T, key_rot.T], axis=0)
    rim_rows = shifted(gated_input[tok_rows - (KERNEL + 1) :], "sp", 1)
    conv_out = convolve(gated_input, rim_rows, conv_taps)
    moment_one, moment_two = lax.psum(
        (jnp.sum(conv_out, axis=1), jnp.sum(conv_out * conv_out, axis=1)), "tp"
    )
    mean_val = moment_one / CONV_CH
    spread = moment_two / CONV_CH - mean_val * mean_val
    normed = (conv_out - mean_val[:, None]) * lax.rsqrt(spread + norm_eps)[:, None]
    swished = jax.nn.silu(normed * conv_ln_gain[None, :] + conv_ln_bias[None, :])
    lat_all = lax.all_gather(packed, "sp", axis=0)
    attended = gathered_attention(q_heads, lat_all, key_up.T, value_up.T).astype(jnp.float32)
    att_sq, conv_sq = lax.psum(
        (
            jnp.sum(attended * attended, axis=1, keepdims=True),
            jnp.sum(swished * swished, axis=1, keepdims=True),
        ),
        "tp",
    )
    att_mixed = (
        attended * lax.rsqrt(att_sq / ATT_WIDTH + norm_eps) * att_out_gain[None, :]
    ).astype(jnp.bfloat16)
    conv_mixed = (
        swished * lax.rsqrt(conv_sq / CONV_CH + norm_eps) * conv_out_gain[None, :]
    ).astype(jnp.bfloat16)
    share = (
        jnp.dot(att_mixed, att_out_weight, preferred_element_type=jnp.float32)
        + jnp.dot(conv_mixed, conv_out_weight, preferred_element_type=jnp.float32)
    ).astype(jnp.bfloat16)
    return lax.psum_scatter(share, "tp", scatter_dimension=1, tiled=True)


def solution(mesh):
    return jax.shard_map(
        shards,
        mesh=mesh,
        in_specs=(
            P("sp", "tp"),
            P(),
            P(None, "tp"),
            P(None, "tp"),
            P(),
            P(),
            P(),
            P(None, "tp"),
            P(None, "tp"),
            P(None, "tp"),
            P(None, "tp"),
            P(None, "tp"),
            P("tp"),
            P("tp"),
            P("tp"),
            P("tp"),
            P("tp", None),
            P("tp", None),
        ),
        out_specs=P("sp", "tp"),
        check_vma=False,
    )
```

```python
import math

import jax
import jax.numpy as jnp
from jax import lax
from jax.experimental import pallas as pl
from jax.experimental.pallas import tpu as pltpu
from jax.sharding import PartitionSpec as P

D_MODEL = 2048
NOPE_DIM = 64
ROT_DIM = 32
VALUE_DIM = 64
CONV_CH = 1024
KERNEL = 31
ATT_WIDTH = 1024


norm_eps = 1e-06
far_below = -1e30
rope_base = 10000.0


def shifted(block, axis, distance):
    devices = range(lax.axis_size(axis))
    route = [(i - distance, i) for i in devices if i - distance in devices]
    return lax.ppermute(block, axis, route)


def rotary_tables(positions, half_dim):
    frequency = rope_base ** (-jnp.arange(half_dim, dtype=jnp.float32) / half_dim)
    angles = positions.astype(jnp.float32)[:, None] * frequency[None, :]
    return (jnp.cos(angles), jnp.sin(angles))


def rotate_half(values, cos_table, sine_table):
    half_dim = cos_table.shape[-1]
    front_half = values[..., :half_dim]
    back_half = values[..., half_dim:]
    return jnp.concatenate(
        [
            front_half * cos_table - back_half * sine_table,
            back_half * cos_table + front_half * sine_table,
        ],
        axis=-1,
    )


MESH = pl.DeviceIdType.MESH


def push(src, dst, send, recv, target):
    return pltpu.make_async_remote_copy(
        src_ref=src,
        dst_ref=dst,
        send_sem=send,
        recv_sem=recv,
        device_id=target,
        device_id_type=MESH,
    )


def greet(targets):
    barrier = pltpu.get_barrier_semaphore()
    for target in targets:
        pl.semaphore_signal(barrier, inc=1, device_id=target, device_id_type=MESH)
    pl.semaphore_wait(barrier, len(targets))


def other_core():
    return {"sp": lax.axis_index("sp"), "tp": 1 - lax.axis_index("tp")}


def front_kernel(
    tok_ref, gain_ref, kv_gain_ref, cos_ref, sin_ref, taps_ref, ln_gain_ref, ln_bias_ref,
    qw_hbm, qrw_hbm, kvd_hbm, rotw_hbm, cvw_hbm, cgw_hbm,
    q_ref, packed_ref, swish_ref,
    qw, qrw, kvd, rotw, cvw, cgw, scaled, landed, narrow, gated, rim, wide, conv,
    sq_mine, sq_other, w_sem, tok_send, tok_recv, rim_send, rim_recv, sq_send, sq_recv,
):
    mine = lax.axis_index("tp")
    seat = lax.axis_index("sp")
    seats = lax.axis_size("sp")
    rows, width = tok_ref.shape
    heads, _, lanes = q_ref.shape
    loads = [
        pltpu.make_async_copy(src, dst, w_sem.at[index])
        for index, (src, dst) in enumerate(
            (
                (kvd_hbm, kvd), (rotw_hbm, rotw), (cvw_hbm, cvw),
                (cgw_hbm, cgw), (qw_hbm, qw), (qrw_hbm, qrw),
            )
        )
    ]
    for load in loads:
        load.start()
    ahead = {"sp": (seat + 1) % seats, "tp": mine}
    behind = {"sp": (seat + seats - 1) % seats, "tp": mine}
    greet([other_core(), ahead, behind])
    copy = push(tok_ref, landed, tok_send, tok_recv, other_core())
    copy.start()

    def place(block, index):
        cols = pl.ds(pl.multiple_of(index * width, 128), width)
        full = block[...].astype(jnp.float32)
        scaled[:, cols] = (full * gain_ref[:, cols]).astype(jnp.bfloat16)
        return jnp.sum(full * full, axis=1, keepdims=True)

    squares = place(tok_ref, mine)
    copy.wait()
    squares = squares + place(landed, 1 - mine)
    row_scale = lax.rsqrt(squares / (2 * width) + norm_eps)

    def project(weight):
        return jnp.dot(scaled[...], weight[...], preferred_element_type=jnp.float32)

    loads[2].wait()
    loads[3].wait()
    gate = project(cgw) * row_scale
    gated[...] = (project(cvw) * row_scale * jax.nn.sigmoid(gate)).astype(jnp.bfloat16)
    edge = rim.shape[0]
    rim_copy = push(gated.at[pl.ds(rows - edge, edge)], rim, rim_send, rim_recv, ahead)

    @pl.when(seat < seats - 1)
    def _():
        rim_copy.start()

    loads[0].wait()
    loads[1].wait()
    raw = project(kvd)
    rank = raw.shape[1]
    latent = (
        raw
        * lax.rsqrt(jnp.mean(raw * raw, axis=1, keepdims=True) + norm_eps)
        * kv_gain_ref[...]
    )
    packed_ref[:rank, :] = latent.T.astype(jnp.bfloat16)
    cos_table = cos_ref[...]
    sin_table = sin_ref[...]
    turn = cos_table.shape[0]

    def rotate(block):
        front = block[:turn]
        back = block[turn : 2 * turn]
        return jnp.concatenate(
            [front * cos_table - back * sin_table, back * cos_table + front * sin_table], axis=0
        )

    narrow[...] = jnp.broadcast_to(row_scale, narrow.shape)
    key_turn = lax.dot_general(
        rotw[...], scaled[...], (((1,), (1,)), ((), ())), preferred_element_type=jnp.float32
    )
    packed_ref[rank:, :] = rotate(key_turn * narrow[...].T[: 2 * turn]).astype(jnp.bfloat16)
    loads[4].wait()
    loads[5].wait()
    query_scale = row_scale * (math.log2(math.e) / math.sqrt(NOPE_DIM + ROT_DIM))
    plain = (project(qw) * query_scale).T
    turned = (project(qrw) * query_scale).T
    blank = jnp.zeros((lanes - NOPE_DIM - ROT_DIM, rows), jnp.float32)
    for head in range(heads):
        column = jnp.concatenate(
            [
                plain[head * NOPE_DIM : (head + 1) * NOPE_DIM],
                rotate(turned[head * ROT_DIM : (head + 1) * ROT_DIM]),
                blank,
            ],
            axis=0,
        )
        q_ref[head] = column.T.astype(jnp.bfloat16)

    @pl.when(seat > 0)
    def _():
        rim_copy.wait_recv()

    @pl.when(seat == 0)
    def _():
        rim[...] = jnp.zeros(rim.shape, jnp.bfloat16)

    taps = taps_ref.shape[0]
    chunk = 64
    for part in range(conv.shape[1] // 128):
        cols = slice(part * 128, (part + 1) * 128)
        wide[part, :edge, :] = rim[:, cols].astype(jnp.float32)
        wide[part, edge:, :] = gated[:, cols].astype(jnp.float32)
        coeff = taps_ref[:, cols]

        def band(step, carry, part=part, cols=cols, coeff=coeff):
            base = step * chunk
            total = jnp.zeros((chunk, 128), jnp.float32)
            for tap in range(taps):
                total = total + coeff[tap : tap + 1, :] * wide[
                    part, pl.ds(base + (edge - taps + 1 + tap), chunk), :
                ]
            conv[pl.ds(pl.multiple_of(base, chunk), chunk), cols] = total
            return carry

        lax.fori_loop(0, rows // chunk, band, 0)

    values = conv[...]
    for slot, total in enumerate((values, values * values)):
        sq_mine[:, slot * 128 : (slot + 1) * 128] = jnp.broadcast_to(
            jnp.sum(total, axis=1, keepdims=True), (rows, 128)
        )
    sums = push(sq_mine, sq_other, sq_send, sq_recv, other_core())
    sums.start()
    sums.wait()
    moments = (sq_mine[...] + sq_other[...]) / CONV_CH
    mean_val = moments[:, :1]
    spread = moments[:, 128:129] - mean_val * mean_val
    normed = (values - mean_val) * lax.rsqrt(spread + norm_eps)
    swish_ref[...] = jax.nn.silu(normed * ln_gain_ref[...] + ln_bias_ref[...])

    @pl.when(seat < seats - 1)
    def _():
        rim_copy.wait_send()


def front(tokens, gain, kv_gain, cos_t, sin_t, taps, ln_gain, ln_bias, weights):
    rows, width = tokens.shape
    chans = taps.shape[1]
    heads = weights[0].shape[1] // NOPE_DIM
    rank = weights[2].shape[1]
    vmem = pl.BlockSpec(memory_space=pltpu.VMEM)
    anywhere = pl.BlockSpec(memory_space=pltpu.HBM)
    dma = pltpu.SemaphoreType.DMA
    edge = 32
    return pl.pallas_call(
        front_kernel,
        out_shape=(
            jax.ShapeDtypeStruct((heads, rows, 128), jnp.bfloat16),
            jax.ShapeDtypeStruct((rank + ROT_DIM, rows), jnp.bfloat16),
            jax.ShapeDtypeStruct((rows, chans), jnp.float32),
        ),
        in_specs=[vmem] * 8 + [anywhere] * 6,
        out_specs=(vmem,) * 3,
        scratch_shapes=[pltpu.VMEM(weight.shape, jnp.bfloat16) for weight in weights]
        + [
            pltpu.VMEM((rows, 2 * width), jnp.bfloat16),
            pltpu.VMEM((rows, width), jnp.bfloat16),
            pltpu.VMEM((rows, 128), jnp.float32),
            pltpu.VMEM((rows, chans), jnp.bfloat16),
            pltpu.VMEM((edge, chans), jnp.bfloat16),
            pltpu.VMEM((chans // 128, rows + edge, 128), jnp.float32),
            pltpu.VMEM((rows, chans), jnp.float32),
            pltpu.VMEM((rows, 256), jnp.float32),
            pltpu.VMEM((rows, 256), jnp.float32),
            dma((6,)),
        ]
        + [dma] * 6,
        compiler_params=pltpu.CompilerParams(
            vmem_limit_bytes=62 << 20, collective_id=0, has_side_effects=True
        ),
        name="front",
    )(tokens, gain, kv_gain, cos_t, sin_t, taps, ln_gain, ln_bias, *weights)


def output_kernel(
    att_ref, swish_ref, att_gain, conv_gain, att_hbm, conv_hbm, out_ref,
    att_w, conv_w, sq_mine, sq_other, part, landed, w_sem, sq_send, sq_recv, send, recv,
):
    loads = [
        pltpu.make_async_copy(att_hbm, att_w, w_sem.at[0]),
        pltpu.make_async_copy(conv_hbm, conv_w, w_sem.at[1]),
    ]
    for load in loads:
        load.start()
    mine = lax.axis_index("tp")
    rows, width = out_ref.shape
    lanes = sq_mine.shape[1] // 2
    attended = att_ref[...].astype(jnp.float32)
    swished = swish_ref[...]
    for slot, value in enumerate((attended, swished)):
        total = jnp.sum(value * value, axis=1, keepdims=True)
        sq_mine[:, slot * lanes : (slot + 1) * lanes] = jnp.broadcast_to(total, (rows, lanes))
    greet([other_core()])
    sums = push(sq_mine, sq_other, sq_send, sq_recv, other_core())
    sums.start()
    sums.wait()
    sq = sq_mine[...] + sq_other[...]
    att_scale = lax.rsqrt(sq[:, :1] / ATT_WIDTH + norm_eps)
    conv_scale = lax.rsqrt(sq[:, lanes : lanes + 1] / CONV_CH + norm_eps)
    att_mixed = (attended * att_scale * att_gain[...]).astype(jnp.bfloat16)
    conv_mixed = (swished * conv_scale * conv_gain[...]).astype(jnp.bfloat16)
    piece = part.shape[2]
    pieces = part.shape[0]

    def product(owner, index):
        cols = pl.ds(pl.multiple_of(owner * width + index * piece, 128), piece)
        return (
            jnp.dot(att_mixed, att_w[:, cols], preferred_element_type=jnp.float32)
            + jnp.dot(conv_mixed, conv_w[:, cols], preferred_element_type=jnp.float32)
        ).astype(jnp.bfloat16)

    for load in loads:
        load.wait()
    copies = []
    for index in range(pieces):
        part[index] = product(1 - mine, index)
        copy = push(
            part.at[index], landed.at[index], send.at[index], recv.at[index], other_core()
        )
        copy.start()
        copies.append(copy)
    for index in range(pieces):
        own = product(mine, index).astype(jnp.float32)
        copies[index].wait()
        out_ref[:, index * piece : (index + 1) * piece] = (
            own + landed[index].astype(jnp.float32)
        ).astype(jnp.bfloat16)


def merge(attended, swished, att_gain, conv_gain, att_w, conv_w):
    rows = attended.shape[0]
    width = att_w.shape[1] // 2
    pieces = 4
    vmem = pl.BlockSpec(memory_space=pltpu.VMEM)
    return pl.pallas_call(
        output_kernel,
        out_shape=jax.ShapeDtypeStruct((rows, width), jnp.bfloat16),
        in_specs=[vmem] * 4 + [pl.BlockSpec(memory_space=pltpu.HBM)] * 2,
        out_specs=vmem,
        scratch_shapes=[
            pltpu.VMEM(att_w.shape, jnp.bfloat16),
            pltpu.VMEM(conv_w.shape, jnp.bfloat16),
            pltpu.VMEM((rows, 256), jnp.float32),
            pltpu.VMEM((rows, 256), jnp.float32),
            pltpu.VMEM((pieces, rows, width // pieces), jnp.bfloat16),
            pltpu.VMEM((pieces, rows, width // pieces), jnp.bfloat16),
            pltpu.SemaphoreType.DMA((2,)),
            pltpu.SemaphoreType.DMA,
            pltpu.SemaphoreType.DMA,
            pltpu.SemaphoreType.DMA((pieces,)),
            pltpu.SemaphoreType.DMA((pieces,)),
        ],
        compiler_params=pltpu.CompilerParams(collective_id=1, has_side_effects=True),
        name="output_merge",
    )(attended, swished, att_gain, conv_gain, att_w, conv_w)


PLANE = 4


def attention_kernel(
    q_ref, own_ref, kup_ref, vup_ref, o_ref, kt, vt, run_max, acc, lat_ref,
    col_send, plane_send, core_send, link_recv, core_recv,
):
    heads, rows, lanes = q_ref.shape
    blocks = lat_ref.shape[0]
    rank = kup_ref.shape[1]
    nope = kup_ref.shape[0] // heads
    vdim = vup_ref.shape[0] // heads
    rot = lat_ref.shape[1] - rank
    wide = kt.shape[2]
    pairing = wide // rows
    me = lax.axis_index("sp")
    core = lax.axis_index("tp")
    layers = blocks // PLANE
    layer = me // PLANE
    spot = me % PLANE
    height = lat_ref.shape[1] // 2
    half = pl.ds(pl.multiple_of(core * height, 16), height)

    def spot_at(distance):
        return (spot + distance) % PLANE

    def at(layer_id, spot_id):
        return {"sp": layer_id * PLANE + spot_id, "tp": core}

    greet(
        [at((layer + d) % layers, spot) for d in range(1, layers)]
        + [at(layer, spot_at(d)) for d in range(1, PLANE)]
        + [other_core()]
    )

    def column_copy(distance):
        return push(
            own_ref.at[half],
            lat_ref.at[me, half],
            col_send.at[distance - 1],
            link_recv.at[me],
            at(jnp.minimum(layer + distance, layers - 1), spot),
        )

    def plane_copy(source, block, distance):
        return push(
            source,
            lat_ref.at[block, half],
            plane_send.at[block // PLANE, distance - 1],
            link_recv.at[block],
            at(layer, spot_at(distance)),
        )

    def core_copy(block):
        spread = lat_ref.at[block, half]
        return push(spread, spread, core_send.at[block], core_recv.at[block], other_core())

    for d in range(1, PLANE):
        plane_copy(own_ref.at[half], me, d).start()
    for d in range(1, layers):

        @pl.when(layer + d < layers)
        def _(d=d):
            column_copy(d).start()

    lat_ref[me] = own_ref[...]

    def relay(step):
        @pl.when(step <= layer)
        def _():
            block = (layer - step) * PLANE + spot
            landed(block)
            for d in range(1, PLANE):
                plane_copy(lat_ref.at[block, half], block, d).start()
            core_copy(block).start()

    def hand_over(step):
        @pl.when(step <= layer)
        def _():
            for d in range(1, PLANE):
                block = (layer - step) * PLANE + spot_at(d)
                landed(block)
                core_copy(block).start()

    def landed(block):
        spread = lat_ref.at[block, half]
        push(spread, spread, core_send.at[block], link_recv.at[block], other_core()).wait_recv()

    def gathered(step):
        for d in range(1, PLANE):
            core_copy((layer - step) * PLANE + spot_at(d)).wait_recv()

    def expand(pair):
        for part in range(pairing):
            src = pair * pairing + part
            lat = lat_ref[src, :rank, :]
            turned = lat_ref[src, rank:, :]
            cols = slice(part * rows, (part + 1) * rows)
            keys = jnp.dot(kup_ref[...], lat, preferred_element_type=jnp.float32)
            values = jnp.dot(vup_ref[...], lat, preferred_element_type=jnp.float32)
            for head in range(heads):
                kt[head, :nope, cols] = keys[head * nope : (head + 1) * nope].astype(jnp.bfloat16)
                kt[head, nope : nope + rot, cols] = turned
                vt[head, :vdim, cols] = values[head * vdim : (head + 1) * vdim].astype(
                    jnp.bfloat16
                )

    def score(head):
        return jnp.dot(q_ref[head], kt[head], preferred_element_type=jnp.float32)

    def weigh(head, scores, top):
        weights = jnp.exp2(scores - top).astype(jnp.bfloat16)
        return lax.dot_general(
            weights, vt[head], (((1,), (1,)), ((), ())), preferred_element_type=jnp.float32
        )

    def visit(group, middle):
        expand(group)
        ahead = score(0)
        for head in range(heads):
            if head == heads // 2:
                middle()
            scores = ahead
            if head + 1 < heads:
                ahead = score(head + 1)
            old = run_max[head]
            top = jnp.maximum(old[:, :1], jnp.max(scores, axis=1, keepdims=True))
            wide_top = jnp.broadcast_to(top, (rows, lanes))
            run_max[head] = wide_top
            acc[head] = acc[head] * jnp.exp2(old - wide_top) + weigh(head, scores, top)

    kt[:, nope + rot :, :] = jnp.zeros((heads, lanes - nope - rot, wide), jnp.bfloat16)
    vt[:, vdim:, :] = jnp.ones((heads, lanes - vdim, wide), jnp.bfloat16)
    hand_over(0)
    relay(1)
    gathered(0)
    expand(layer)
    key_pos = layer * wide + lax.broadcasted_iota(jnp.int32, (rows, wide), 1)
    query_pos = me * rows + lax.broadcasted_iota(jnp.int32, (rows, wide), 0)
    hidden = key_pos > query_pos
    ahead = score(0)
    for head in range(heads):
        if head == heads // 2:
            hand_over(1)
            relay(2)
        scores = jnp.where(hidden, far_below, ahead)
        if head + 1 < heads:
            ahead = score(head + 1)
        top = jnp.max(scores, axis=1, keepdims=True)
        run_max[head] = jnp.broadcast_to(top, (rows, lanes))
        acc[head] = weigh(head, scores, top)

    def far(step, carry):
        for d in range(PLANE):
            core_copy((layer - step) * PLANE + spot_at(d)).wait_recv()

        def middle():
            hand_over(step + 1)
            relay(step + 2)

        visit(layer - step, middle)
        return carry

    lax.fori_loop(1, layer + 1, far, 0)
    lane = lax.broadcasted_iota(jnp.int32, (rows, lanes), 1)
    for pair in range(heads // 2):
        halves = []
        for head in (2 * pair, 2 * pair + 1):
            total = acc[head]
            halves.append(total / pltpu.roll(total, vdim, axis=1))
        both = jnp.where(lane < vdim, halves[0], pltpu.roll(halves[1], vdim, axis=1))
        o_ref[:, pair * lanes : (pair + 1) * lanes] = both.astype(jnp.bfloat16)

    for d in range(1, layers):

        @pl.when(layer + d < layers)
        def _(d=d):
            column_copy(d).wait_send()

    def settle(step, carry):
        base = (layer - step) * PLANE
        for d in range(1, PLANE):
            plane_copy(own_ref.at[half], base + spot, d).wait_send()
            core_copy(base + spot_at(d)).wait_send()

        @pl.when(step > 0)
        def _():
            core_copy(base + spot).wait_send()

        return carry

    lax.fori_loop(0, layer + 1, settle, 0)


def attention(q_heads, packed, key_up_t, value_up_t):
    heads, rows, lanes = q_heads.shape
    blocks = lax.axis_size("sp")
    wide = PLANE * rows
    layers = blocks // PLANE
    vmem = pl.BlockSpec(memory_space=pltpu.VMEM)
    dma = pltpu.SemaphoreType.DMA
    return pl.pallas_call(
        attention_kernel,
        out_shape=jax.ShapeDtypeStruct((rows, value_up_t.shape[0]), jnp.bfloat16),
        in_specs=[vmem] * 4,
        out_specs=vmem,
        scratch_shapes=[
            pltpu.VMEM((heads, lanes, wide), jnp.bfloat16),
            pltpu.VMEM((heads, lanes, wide), jnp.bfloat16),
            pltpu.VMEM((heads, rows, lanes), jnp.float32),
            pltpu.VMEM((heads, rows, lanes), jnp.float32),
            pltpu.VMEM((blocks,) + packed.shape, jnp.bfloat16),
            dma((max(layers - 1, 1),)),
            dma((layers, PLANE - 1)),
            dma((blocks,)),
            dma((blocks,)),
            dma((blocks,)),
        ],
        compiler_params=pltpu.CompilerParams(
            vmem_limit_bytes=40 << 20, collective_id=2, has_side_effects=True
        ),
        name="attention",
    )(q_heads, packed, key_up_t, value_up_t)


def gathered_kernel(q_ref, lat_ref, kup_ref, vup_ref, o_ref, kt, vt, run_max, acc):
    heads, rows, lanes = q_ref.shape
    blocks = lat_ref.shape[0]
    rank = kup_ref.shape[1]
    nope = kup_ref.shape[0] // heads
    vdim = vup_ref.shape[0] // heads
    rot = lat_ref.shape[1] - rank
    wide = kt.shape[2]
    group = wide // rows
    me = lax.axis_index("sp")
    last = me // group
    kt[:, nope + rot :, :] = jnp.zeros((heads, lanes - nope - rot, wide), jnp.bfloat16)
    vt[:, vdim:, :] = jnp.ones((heads, lanes - vdim, wide), jnp.bfloat16)

    def expand(block):
        for part in range(group):
            src = jnp.minimum(block * group + part, blocks - 1)
            lat = lat_ref[src, :rank, :]
            turned = lat_ref[src, rank:, :]
            cols = slice(part * rows, (part + 1) * rows)
            keys = jnp.dot(kup_ref[...], lat, preferred_element_type=jnp.float32)
            values = jnp.dot(vup_ref[...], lat, preferred_element_type=jnp.float32)
            for head in range(heads):
                kt[head, :nope, cols] = keys[head * nope : (head + 1) * nope].astype(jnp.bfloat16)
                kt[head, nope : nope + rot, cols] = turned
                vt[head, :vdim, cols] = values[head * vdim : (head + 1) * vdim].astype(
                    jnp.bfloat16
                )

    def weigh(head, scores, top):
        weights = jnp.exp2(scores - top).astype(jnp.bfloat16)
        return lax.dot_general(
            weights, vt[head], (((1,), (1,)), ((), ())), preferred_element_type=jnp.float32
        )

    expand(last)
    key_pos = last * wide + lax.broadcasted_iota(jnp.int32, (rows, wide), 1)
    query_pos = me * rows + lax.broadcasted_iota(jnp.int32, (rows, wide), 0)
    hidden = key_pos > query_pos
    for head in range(heads):
        scores = jnp.dot(q_ref[head], kt[head], preferred_element_type=jnp.float32)
        scores = jnp.where(hidden, far_below, scores)
        top = jnp.max(scores, axis=1, keepdims=True)
        run_max[head] = jnp.broadcast_to(top, (rows, lanes))
        acc[head] = weigh(head, scores, top)

    def visit(step, carry):
        expand(step)
        for head in range(heads):
            scores = jnp.dot(q_ref[head], kt[head], preferred_element_type=jnp.float32)
            old = run_max[head]
            top = jnp.maximum(old[:, :1], jnp.max(scores, axis=1, keepdims=True))
            wide_top = jnp.broadcast_to(top, (rows, lanes))
            run_max[head] = wide_top
            acc[head] = acc[head] * jnp.exp2(old - wide_top) + weigh(head, scores, top)
        return carry

    lax.fori_loop(0, last, visit, 0)
    lane = lax.broadcasted_iota(jnp.int32, (rows, lanes), 1)
    for pair in range(heads // 2):
        halves = []
        for head in (2 * pair, 2 * pair + 1):
            total = acc[head]
            halves.append(total / pltpu.roll(total, vdim, axis=1))
        both = jnp.where(lane < vdim, halves[0], pltpu.roll(halves[1], vdim, axis=1))
        o_ref[:, pair * lanes : (pair + 1) * lanes] = both.astype(jnp.bfloat16)


def gathered_attention(q_heads, lat_all, key_up_t, value_up_t):
    heads, rows, lanes = q_heads.shape
    blocks = lat_all.shape[0]
    wide = 2 * rows if blocks % 2 == 0 else rows
    vmem = pl.BlockSpec(memory_space=pltpu.VMEM)
    return pl.pallas_call(
        gathered_kernel,
        out_shape=jax.ShapeDtypeStruct((rows, value_up_t.shape[0]), jnp.bfloat16),
        in_specs=[vmem] * 4,
        out_specs=vmem,
        scratch_shapes=[
            pltpu.VMEM((heads, lanes, wide), jnp.bfloat16),
            pltpu.VMEM((heads, lanes, wide), jnp.bfloat16),
            pltpu.VMEM((heads, rows, lanes), jnp.float32),
            pltpu.VMEM((heads, rows, lanes), jnp.float32),
        ],
        compiler_params=pltpu.CompilerParams(vmem_limit_bytes=48 << 20),
        cost_estimate=pl.CostEstimate(
            flops=20_000_000_000, bytes_accessed=8 << 20, transcendentals=20_000_000
        ),
        name="gathered_attention",
    )(q_heads, lat_all, key_up_t, value_up_t)


def conv_kernel(gated_ref, rim_ref, taps_ref, out_ref, wide):
    rows, chans = gated_ref.shape
    rim = rim_ref.shape[0]
    taps = taps_ref.shape[0]
    chunk = 64
    for part in range(chans // 128):
        cols = slice(part * 128, (part + 1) * 128)
        wide[part, :rim, :] = rim_ref[:, cols].astype(jnp.float32)
        wide[part, rim:, :] = gated_ref[:, cols].astype(jnp.float32)
        coeff = taps_ref[:, cols]

        def band(step, carry):
            base = step * chunk
            total = jnp.zeros((chunk, 128), jnp.float32)
            for tap in range(taps):
                total = total + coeff[tap : tap + 1, :] * wide[
                    part, pl.ds(base + (rim - taps + 1 + tap), chunk), :
                ]
            out_ref[pl.ds(pl.multiple_of(base, chunk), chunk), cols] = total
            return carry

        lax.fori_loop(0, rows // chunk, band, 0)


def convolve(gated, rim, taps):
    rows, chans = gated.shape
    vmem = pl.BlockSpec(memory_space=pltpu.VMEM)
    return pl.pallas_call(
        conv_kernel,
        out_shape=jax.ShapeDtypeStruct((rows, chans), jnp.float32),
        in_specs=[vmem] * 3,
        out_specs=vmem,
        scratch_shapes=[pltpu.VMEM((chans // 128, rows + rim.shape[0], 128), jnp.float32)],
        cost_estimate=pl.CostEstimate(
            flops=2 * rows * chans * 31, bytes_accessed=2 << 20, transcendentals=0
        ),
        name="depthwise",
    )(gated, rim, taps)


def shards(
    tokens,
    input_gain,
    query_weight,
    query_rot_weight,
    kv_down,
    rot_down,
    kv_gain,
    key_up,
    value_up,
    conv_value_weight,
    conv_gate_weight,
    conv_taps,
    conv_ln_gain,
    conv_ln_bias,
    att_out_gain,
    conv_out_gain,
    att_out_weight,
    conv_out_weight,
):
    tok_rows = tokens.shape[0]
    heads_here = key_up.shape[1] // NOPE_DIM
    chan_here = conv_taps.shape[1]
    weight_list = (
        query_weight,
        query_rot_weight,
        kv_down,
        rot_down,
        conv_value_weight,
        conv_gate_weight,
    )
    if lax.axis_size("tp") == 2 and lax.axis_size("sp") % PLANE == 0:
        positions = lax.axis_index("sp") * tok_rows + jnp.arange(tok_rows, dtype=jnp.int32)
        cos_table, sine_table = rotary_tables(positions, ROT_DIM // 2)
        q_heads, packed, swished = front(
            tokens,
            input_gain[None, :],
            kv_gain[None, :],
            cos_table.T,
            sine_table.T,
            conv_taps,
            conv_ln_gain[None, :],
            conv_ln_bias[None, :],
            weight_list[:3] + (rot_down.T,) + weight_list[4:],
        )
        attended = attention(q_heads, packed, key_up.T, value_up.T)
        return merge(
            attended,
            swished,
            att_out_gain[None, :],
            conv_out_gain[None, :],
            att_out_weight,
            conv_out_weight,
        )
    whole_rows = lax.all_gather(tokens, "tp", axis=1, tiled=True).astype(jnp.float32)
    scaled = (whole_rows * input_gain[None, :]).astype(jnp.bfloat16)
    row_scale = lax.rsqrt(jnp.mean(whole_rows * whole_rows, axis=1, keepdims=True) + norm_eps)

    def add_product(weight):
        return jnp.dot(scaled, weight, preferred_element_type=jnp.float32)

    summed = tuple((add_product(weight) for weight in weight_list))
    q_acc, qrot_acc, latent_raw, rot_acc, value_acc, gate_acc = summed
    positions = lax.axis_index("sp") * tok_rows + jnp.arange(tok_rows, dtype=jnp.int32)
    cos_table, sine_table = rotary_tables(positions, ROT_DIM // 2)
    fold = math.log2(math.e) / math.sqrt(NOPE_DIM + ROT_DIM)
    query_scale = row_scale * fold
    plain_q = (q_acc * query_scale).reshape(tok_rows, heads_here, NOPE_DIM)
    turned_q = rotate_half(
        (qrot_acc * query_scale).reshape(tok_rows, heads_here, ROT_DIM),
        cos_table[:, None, :],
        sine_table[:, None, :],
    )
    blank = jnp.zeros((tok_rows, heads_here, 128 - NOPE_DIM - ROT_DIM), jnp.float32)
    q_heads = jnp.transpose(
        jnp.concatenate([plain_q, turned_q, blank], axis=2).astype(jnp.bfloat16), (1, 0, 2)
    )
    latent = (
        latent_raw
        * lax.rsqrt(jnp.mean(latent_raw * latent_raw, axis=1, keepdims=True) + norm_eps)
        * kv_gain[None, :]
    ).astype(jnp.bfloat16)
    key_rot = rotate_half(rot_acc * row_scale, cos_table, sine_table).astype(jnp.bfloat16)
    gated_input = (value_acc * row_scale * jax.nn.sigmoid(gate_acc * row_scale)).astype(
        jnp.bfloat16
    )
    packed = jnp.concatenate([latent.T, key_rot.T], axis=0)
    rim_rows = shifted(gated_input[tok_rows - (KERNEL + 1) :], "sp", 1)
    conv_out = convolve(gated_input, rim_rows, conv_taps)
    moment_one, moment_two = lax.psum(
        (jnp.sum(conv_out, axis=1), jnp.sum(conv_out * conv_out, axis=1)), "tp"
    )
    mean_val = moment_one / CONV_CH
    spread = moment_two / CONV_CH - mean_val * mean_val
    normed = (conv_out - mean_val[:, None]) * lax.rsqrt(spread + norm_eps)[:, None]
    swished = jax.nn.silu(normed * conv_ln_gain[None, :] + conv_ln_bias[None, :])
    lat_all = lax.all_gather(packed, "sp", axis=0)
    attended = gathered_attention(q_heads, lat_all, key_up.T, value_up.T).astype(jnp.float32)
    att_sq, conv_sq = lax.psum(
        (
            jnp.sum(attended * attended, axis=1, keepdims=True),
            jnp.sum(swished * swished, axis=1, keepdims=True),
        ),
        "tp",
    )
    att_mixed = (
        attended * lax.rsqrt(att_sq / ATT_WIDTH + norm_eps) * att_out_gain[None, :]
    ).astype(jnp.bfloat16)
    conv_mixed = (
        swished * lax.rsqrt(conv_sq / CONV_CH + norm_eps) * conv_out_gain[None, :]
    ).astype(jnp.bfloat16)
    share = (
        jnp.dot(att_mixed, att_out_weight, preferred_element_type=jnp.float32)
        + jnp.dot(conv_mixed, conv_out_weight, preferred_element_type=jnp.float32)
    ).astype(jnp.bfloat16)
    return lax.psum_scatter(share, "tp", scatter_dimension=1, tiled=True)


def solution(mesh):
    return jax.shard_map(
        shards,
        mesh=mesh,
        in_specs=(
            P("sp", "tp"),
            P(),
            P(None, "tp"),
            P(None, "tp"),
            P(),
            P(),
            P(),
            P(None, "tp"),
            P(None, "tp"),
            P(None, "tp"),
            P(None, "tp"),
            P(None, "tp"),
            P("tp"),
            P("tp"),
            P("tp"),
            P("tp"),
            P("tp", None),
            P("tp", None),
        ),
        out_specs=P("sp", "tp"),
        check_vma=False,
    )
```
